32 devices in a mesh: sp: 8 (over z, x), tp: 4 (over y, core).
Axes of the slice: x: 2, y: 2, z: 4, core: 2. Of those that a mesh axis runs over, the one named last changes fastest.
Arguments:
- tokens: bfloat16 [2048, 2048], P(('sp', 'tp')), may hold values from -6 to 6
- norm_gain: float32 [2048], replicated, may hold values from 0.1 to 1.9
- w_glu_a: bfloat16 [2048, 2048], P(None, 'tp'), may hold values from -0.125 to 0.125
- w_glu_b: bfloat16 [2048, 2048], P(None, 'tp'), may hold values from -0.125 to 0.125
- conv_taps: float32 [31, 2048], P(None, 'tp'), may hold values from -6 to 6
- ln_gain: float32 [2048], P('tp'), may hold values from 0.1 to 1.9
- w_query: bfloat16 [2048, 2048], P(None, 'tp'), may hold values from -0.125 to 0.125
- w_key: bfloat16 [2048, 512], P(None, 'tp'), may hold values from -0.125 to 0.125
- w_value: bfloat16 [2048, 512], P(None, 'tp'), may hold values from -0.125 to 0.125
- query_gain: float32 [16, 128], P('tp'), may hold values from 1 to 40
- key_gain: float32 [4, 128], P('tp'), may hold values from 0.1 to 1.9
- lam_head: float32 [16], P('tp'), may hold values from 0.3 to 0.8
- sub_gain: float32 [128], replicated, may hold values from 0.1 to 1.9
- w_out_conv: bfloat16 [2048, 2048], P('tp'), may hold values from -0.09375 to 0.09375
- w_out_attn: bfloat16 [2048, 2048], P('tp'), may hold values from -0.09375 to 0.09375
Outputs:
- mixed: bfloat16 [2048, 2048], P(('sp', 'tp'))
- log_sums: float32 [2, 16, 2048], P(None, 'tp', 'sp')
The draws below stay inside these ranges and needn't reach their ends.
All inputs are finite; a program needn't handle non-finite values.
Results may differ from the reference program's by a relative error of at most 0.015.
The reference program's roundings to bfloat16 on the way count: a program that leaves them out, or rounds other values in their place, can miss the bound.
Values may be sent and summed in bfloat16 or wider, within the bound.
A program may use at most 128 MiB of HBM per device.

```python
import jax
import jax.numpy as jnp
from jax import lax

D = 2048
CONV_CH = 2048
KW = 31
HEADS = 16
KV_HEADS = 4
HEAD_DIM = 64
VALUE_DIM = 128
TOKENS = 2048
N_TP = 4


def draw_conv_taps(key, part):
    normal_part = jax.random.truncated_normal(key, -3.0, 3.0, (KW, CONV_CH), jnp.float32)
    channel_pos = jnp.arange(CONV_CH, dtype=jnp.float32) / CONV_CH
    growth = 3.0
    return normal_part * KW ** (-0.5) * jnp.exp(jnp.log(growth) * channel_pos)[None, :]


def draw_query_gain(key, part):
    gains = jax.random.uniform(key, (HEADS, 2 * HEAD_DIM), jnp.float32, 1.2, 1.9)
    return gains


def level_of(rng, extent, pieces, least, largest):
    def one(axis_at, blocks):
        draws = jax.random.uniform(jax.random.fold_in(jax.random.fold_in(rng, 6), axis_at), (blocks,), jnp.float32, least / len(pieces), largest / len(pieces))
        return jnp.repeat(jnp.exp(draws), extent[axis_at] // blocks).reshape((-1,) + (1,) * (len(extent) - axis_at - 1))

    loudness = one(*pieces[0])
    for cut in pieces[1:]:
        loudness = loudness * one(*cut)
    return loudness


def normal_values(key, shape, scale, reach, cuts=(), kind=jnp.bfloat16):
    factor_of = level_of(key, shape, cuts, -0.22, 0.18) if cuts else 1.0
    drawn = jax.random.normal(key, shape, jnp.float32) * scale * factor_of
    return jnp.minimum(jnp.maximum(drawn, -reach), reach).astype(kind)


def setup_inputs(seed: int = 0) -> dict:
    key_list = jax.random.split(jax.random.key(seed), 16)
    return {
        "tokens": normal_values(key_list[0], (TOKENS, D), 1.0, 6.0, ((0, 32),)),
        "norm_gain": jnp.clip(1.0 + 0.18 * jax.random.normal(key_list[1], (D,), jnp.float32), 0.1, 1.9),
        "w_glu_a": normal_values(key_list[2], (D, CONV_CH), D ** -0.5, 0.125, ((1, 4),)),
        "w_glu_b": normal_values(key_list[3], (D, CONV_CH), D ** -0.5, 0.125, ((1, 4),)),
        "conv_taps": draw_conv_taps(jax.random.fold_in(key_list[15], 71), 0),
        "ln_gain": jnp.clip(1.0 + 0.18 * jax.random.normal(key_list[5], (CONV_CH,), jnp.float32), 0.1, 1.9),
        "w_query": normal_values(key_list[6], (D, HEADS * 2 * HEAD_DIM), D ** -0.5, 0.125, ((1, 4),)),
        "w_key": normal_values(key_list[7], (D, KV_HEADS * 2 * HEAD_DIM), D ** -0.5, 0.125, ((1, 4),)),
        "w_value": normal_values(key_list[8], (D, KV_HEADS * VALUE_DIM), D ** -0.5, 0.125, ((1, 4),)),
        "query_gain": draw_query_gain(jax.random.fold_in(key_list[15], 71), 0),
        "key_gain": jnp.clip(1.0 + 0.18 * jax.random.normal(key_list[10], (KV_HEADS, 2 * HEAD_DIM), jnp.float32), 0.1, 1.9),
        "lam_head": jnp.clip(0.3 + 0.5 * jax.random.uniform(key_list[11], (HEADS,), jnp.float32) ** level_of(key_list[11], (HEADS,), ((0, 4),), -0.2, 0.2), 0.3, 0.8),
        "sub_gain": jnp.clip(1.0 + 0.18 * jax.random.normal(key_list[12], (VALUE_DIM,), jnp.float32), 0.1, 1.9),
        "w_out_conv": normal_values(key_list[13], (CONV_CH, D), (CONV_CH + HEADS * VALUE_DIM) ** -0.5, 0.09375, ((0, 4),)),
        "w_out_attn": normal_values(key_list[14], (HEADS * VALUE_DIM, D), (CONV_CH + HEADS * VALUE_DIM) ** -0.5, 0.09375, ((0, 4),)),
    }


def rms_scale(inputs_arr, gain_vec, epsilon):
    return inputs_arr * lax.rsqrt(lax.optimization_barrier(jnp.mean(inputs_arr * inputs_arr, axis=-1, keepdims=True)) + epsilon) * gain_vec

def reference(tokens, norm_gain, w_glu_a, w_glu_b, conv_taps, ln_gain, w_query, w_key, w_value, query_gain, key_gain, lam_head, sub_gain, w_out_conv, w_out_attn):
    seq_len = tokens.shape[0]
    normed = rms_scale(tokens.astype(jnp.float32), norm_gain, 1e-06).astype(jnp.bfloat16)
    glu_a = jnp.dot(normed, w_glu_a, preferred_element_type=jnp.float32)
    glu_b = jnp.dot(normed, w_glu_b, preferred_element_type=jnp.float32)
    gated_rows = (glu_a * jax.nn.sigmoid(glu_b)).astype(jnp.bfloat16)
    padded = jnp.concatenate([jnp.zeros((KW - 1, CONV_CH), jnp.bfloat16), gated_rows], axis=0)
    conv_sum = jnp.zeros((seq_len, CONV_CH), jnp.float32)
    for tap_idx in range(KW):
        conv_sum = conv_sum + conv_taps[tap_idx] * padded[tap_idx:tap_idx + seq_len].astype(jnp.float32)
    mean_val = lax.optimization_barrier(jnp.mean(conv_sum, axis=1, keepdims=True))
    mean_sq = lax.optimization_barrier(jnp.mean(conv_sum * conv_sum, axis=1, keepdims=True))
    normed_conv = (conv_sum - mean_val) * lax.rsqrt(mean_sq - mean_val * mean_val + 1e-05) * ln_gain
    conv_out = jax.nn.silu(normed_conv).astype(jnp.bfloat16)
    queries = jnp.dot(normed, w_query, preferred_element_type=jnp.float32).reshape(seq_len, HEADS, 2, HEAD_DIM)
    queries = rms_scale(queries, query_gain.reshape(HEADS, 2, HEAD_DIM), 1e-06).astype(jnp.bfloat16)
    key_heads = jnp.dot(normed, w_key, preferred_element_type=jnp.float32).reshape(seq_len, KV_HEADS, 2, HEAD_DIM)
    key_heads = rms_scale(key_heads, key_gain.reshape(KV_HEADS, 2, HEAD_DIM), 1e-06).astype(jnp.bfloat16)
    value_heads = jnp.dot(normed, w_value, preferred_element_type=jnp.float32).astype(jnp.bfloat16).reshape(seq_len, KV_HEADS, VALUE_DIM)
    group_size = HEADS // KV_HEADS
    query_rows = min(1024, seq_len)
    block_count = seq_len // query_rows
    key_pos = jnp.arange(seq_len, dtype=jnp.int32)

    def one_block(indices):
        head_idx, block_idx = indices
        kv_idx = head_idx // group_size
        row_first = block_idx * query_rows
        query_blk = lax.dynamic_slice(queries, (row_first, head_idx, jnp.int32(0), jnp.int32(0)), (query_rows, 1, 2, HEAD_DIM))[:, 0]
        key_head = lax.dynamic_index_in_dim(key_heads, kv_idx, 1, keepdims=False)
        value_head = lax.dynamic_index_in_dim(value_heads, kv_idx, 1, keepdims=False)
        query_pos = row_first + jnp.arange(query_rows, dtype=jnp.int32)
        visible = key_pos[None, :] <= query_pos[:, None]
        outputs = []
        log_list = []
        for map_idx in range(2):
            scores = jnp.dot(query_blk[:, map_idx], key_head[:, map_idx].T, preferred_element_type=jnp.float32) * HEAD_DIM ** (-0.5)
            scores = jnp.where(visible, scores, -jnp.inf)
            row_max = lax.optimization_barrier(jnp.max(scores, axis=1, keepdims=True))
            weights = jnp.exp(scores - row_max)
            row_total = lax.optimization_barrier(jnp.sum(weights, axis=1, keepdims=True))
            mixed_map = jnp.dot(weights.astype(jnp.bfloat16), value_head, preferred_element_type=jnp.float32) / row_total
            outputs.append(mixed_map)
            log_list.append((row_max + jnp.log(row_total))[:, 0])
        lam_value = lam_head[head_idx]
        diff_out = outputs[0] - lam_value * outputs[1]
        head_out = rms_scale(diff_out, sub_gain, 1e-06).astype(jnp.bfloat16)
        return (head_out, jnp.stack(log_list))
    head_ids = jnp.repeat(jnp.arange(HEADS, dtype=jnp.int32), block_count)
    block_ids = jnp.tile(jnp.arange(block_count, dtype=jnp.int32), HEADS)
    attn_blocks, lse_blocks = lax.map(one_block, (head_ids, block_ids))
    attn_out = attn_blocks.reshape(HEADS, block_count, query_rows, VALUE_DIM).transpose(1, 2, 0, 3).reshape(seq_len, HEADS * VALUE_DIM)
    log_sums = lse_blocks.reshape(HEADS, block_count, 2, query_rows).transpose(2, 0, 1, 3).reshape(2, HEADS, seq_len)
    conv_part = CONV_CH // N_TP
    attn_part = HEADS * VALUE_DIM // N_TP
    mixed_sum = jnp.zeros((seq_len, D), jnp.float32)
    for group_idx in range(N_TP):
        conv_lo = group_idx * conv_part
        attn_lo = group_idx * attn_part
        partial_value = jnp.dot(conv_out[:, conv_lo:conv_lo + conv_part], w_out_conv[conv_lo:conv_lo + conv_part], preferred_element_type=jnp.float32)
        partial_value = partial_value + jnp.dot(attn_out[:, attn_lo:attn_lo + attn_part], w_out_attn[attn_lo:attn_lo + attn_part], preferred_element_type=jnp.float32)
        mixed_sum = mixed_sum + lax.optimization_barrier(partial_value.astype(jnp.bfloat16)).astype(jnp.float32)
    return (mixed_sum.astype(jnp.bfloat16), log_sums)
```

```python
import functools

import jax
import jax.numpy as jnp
from jax import lax
from jax.experimental import pallas as pl
from jax.experimental.pallas import tpu as pltpu
from jax.sharding import PartitionSpec as P

KW = 31
HALO = 32
F32 = jnp.float32
BF16 = jnp.bfloat16
MESH = pl.DeviceIdType.MESH


def dot(a, b):
    return jnp.dot(a, b, preferred_element_type=F32)


def kernel(
    sp_n,
    tp_n,
    tokens_hbm,
    norm_gain_hbm,
    w_glu_a,
    w_glu_b,
    taps_hbm,
    ln_gain_hbm,
    w_query,
    w_key,
    w_value,
    q_gain_hbm,
    k_gain_hbm,
    lam_hbm,
    sub_gain_hbm,
    w_out_conv,
    w_out_attn,
    mixed,
    logs,
    tokens,
    norm_gain,
    taps,
    ln_gain,
    q_gain,
    k_gain,
    lam,
    sub_gain,
    wa,
    wb,
    wq,
    wkv,
    woc,
    woa,
    nrm,
    kv,
    qtz,
    gat,
    halo_s,
    halo_r,
    conv,
    st,
    stat,
    c_out,
    m_ref,
    l_ref,
    acc,
    a_out,
    part,
    mate_s,
    mate_r,
    y_s,
    y_r,
    in_sem,
    w_sem,
    ag_send,
    ag_recv,
    z_send,
    x_send,
    kv_recv,
    halo_sem,
    stat_send,
    stat_recv,
    mate_send,
    mate_recv,
    y_send,
    y_recv,
):
    sp = lax.axis_index("sp")
    tp = lax.axis_index("tp")
    rows = tokens.shape[0]
    width = tokens.shape[1]
    tok = rows * tp_n
    half_rows = tok // 2
    heads = q_gain.shape[0]
    vdim = sub_gain.shape[1]
    hd = q_gain.shape[1] // 2
    chans = taps.shape[1]
    core = tp % 2
    y = tp // 2
    yo = 1 - y
    mate = tp + 1 - 2 * core
    cross = (tp + 2) % 4
    lane = sp % 2
    pos = sp // 2
    npos = sp_n // 2
    xmate = sp + 1 - 2 * lane

    bar = pltpu.get_barrier_semaphore()

    def greet_sp(i, c):
        pl.semaphore_signal(bar, inc=1, device_id=((sp + i) % sp_n, tp), device_id_type=MESH)
        return c

    lax.fori_loop(1, sp_n, greet_sp, 0)
    for i in range(1, tp_n):
        pl.semaphore_signal(bar, inc=1, device_id=(sp, (tp + i) % tp_n), device_id_type=MESH)

    kw = w_key.shape[1]
    smalls = [
        pltpu.make_async_copy(src, dst, in_sem.at[i])
        for i, (src, dst) in enumerate(
            [
                (tokens_hbm, tokens),
                (norm_gain_hbm, norm_gain),
                (k_gain_hbm, k_gain),
                (q_gain_hbm, q_gain),
                (taps_hbm, taps),
                (ln_gain_hbm, ln_gain),
                (sub_gain_hbm, sub_gain),
                (lam_hbm, lam),
            ]
        )
    ]
    for copy in smalls:
        copy.start()
    loads = [
        pltpu.make_async_copy(w_key, wkv.at[:, :kw], w_sem.at[0]),
        pltpu.make_async_copy(w_value, wkv.at[:, kw:], w_sem.at[1]),
        pltpu.make_async_copy(w_glu_a, wa, w_sem.at[2]),
        pltpu.make_async_copy(w_glu_b, wb, w_sem.at[3]),
        pltpu.make_async_copy(w_query, wq, w_sem.at[4]),
        pltpu.make_async_copy(w_out_conv, woc, w_sem.at[5]),
        pltpu.make_async_copy(w_out_attn, woa, w_sem.at[6]),
    ]
    for copy in loads:
        copy.start()

    qtz[...] = jnp.zeros_like(qtz)
    smalls[0].wait()
    smalls[1].wait()
    x = tokens[...].astype(F32)
    scale = lax.rsqrt(jnp.mean(x * x, axis=-1, keepdims=True) + 1e-06)
    nrm[tp] = (x * scale * norm_gain[...]).astype(BF16)
    pl.semaphore_wait(bar, sp_n - 1 + tp_n - 1)

    ag_chunks = 4

    def ag_copy(slot, k, i, target):
        piece = pl.ds(i * (rows // ag_chunks), rows // ag_chunks)
        return pltpu.make_async_remote_copy(
            src_ref=nrm.at[slot, piece],
            dst_ref=nrm.at[slot, piece],
            send_sem=ag_send.at[k, i],
            recv_sem=ag_recv.at[k, i],
            device_id=(sp, target),
            device_id_type=MESH,
        )

    ag_cross = [ag_copy(tp, 0, i, cross) for i in range(ag_chunks)]
    ag_mate = [
        pltpu.make_async_remote_copy(
            src_ref=nrm.at[tp],
            dst_ref=nrm.at[tp],
            send_sem=ag_send.at[1, 0],
            recv_sem=ag_recv.at[1, 0],
            device_id=(sp, mate),
            device_id_type=MESH,
        )
    ]
    ag_fwd = [ag_copy(cross, 2, i, mate) for i in range(ag_chunks)]
    for copy in ag_cross + ag_mate:
        copy.start()

    def half_in(h):
        return nrm[pl.ds(2 * h, 2)].reshape(half_rows, width)

    def proj_kv(h):
        res = dot(half_in(h), wkv[...])
        k = res[:, :kw]
        v = res[:, kw:]
        first = lax.broadcasted_iota(jnp.int32, k.shape, 1) < hd
        sq = k * k
        s0 = jnp.sum(jnp.where(first, sq, 0.0), axis=1, keepdims=True)
        s1 = jnp.sum(jnp.where(first, 0.0, sq), axis=1, keepdims=True)
        r = jnp.where(first, lax.rsqrt(s0 / hd + 1e-06), lax.rsqrt(s1 / hd + 1e-06))
        kv[sp, h, :half_rows, :] = (k * r * k_gain[...]).astype(BF16)
        kv[sp, h, half_rows:, :] = v.T.astype(BF16)

    def z_copy(t, h):
        return pltpu.make_async_remote_copy(
            src_ref=kv.at[sp, h],
            dst_ref=kv.at[sp, h],
            send_sem=z_send.at[t, h],
            recv_sem=kv_recv.at[sp, h],
            device_id=(t * 2 + lane, tp),
            device_id_type=MESH,
        )

    def x_copy(p, h):
        s = p * 2 + lane
        return pltpu.make_async_remote_copy(
            src_ref=kv.at[s, h],
            dst_ref=kv.at[s, h],
            send_sem=x_send.at[p, h],
            recv_sem=kv_recv.at[s, h],
            device_id=(xmate, tp),
            device_id_type=MESH,
        )

    def arrived(s, h):
        pltpu.make_async_remote_copy(
            src_ref=kv.at[s, h],
            dst_ref=kv.at[s, h],
            send_sem=x_send.at[0, h],
            recv_sem=kv_recv.at[s, h],
            device_id=(xmate, tp),
            device_id_type=MESH,
        ).wait_recv()

    def send_kv(h):
        @pl.when(lane == 0)
        def _():
            x_copy(pos, h).start()

        def one(i, c):
            z_copy(npos - 1 - i, h).start()
            return c

        lax.fori_loop(0, npos - 1 - pos, one, 0)

    def relay_kv(h):
        def one(i, c):
            p = pos - 1 - i
            arrived(p * 2 + lane, h)
            x_copy(p, h).start()
            return c

        lax.fori_loop(0, pos, one, 0)

    def proj_glu(h):
        xin = half_in(h)
        wide = 256

        def one(n, c):
            cols = pl.ds(pl.multiple_of(n * wide, wide), wide)
            a = dot(xin, wa[:, cols])
            b = dot(xin, wb[:, cols])
            g = (a * jax.nn.sigmoid(b)).astype(BF16)
            gat[pl.ds(pl.multiple_of(HALO + h * half_rows, HALO), half_rows), cols] = g.astype(F32)

            @pl.when(h == 1)
            def _():
                halo_s[:, cols] = g[half_rows - HALO :, :]

            return c

        lax.fori_loop(0, chans // wide, one, 0)

    def proj_q(h):
        xin = half_in(h)

        def one(n, c):
            q = dot(xin, wq[:, pl.ds(pl.multiple_of(n * 4 * hd, 4 * hd), 4 * hd)])
            qt = q.T.reshape(4, hd, half_rows)
            r = lax.rsqrt(jnp.mean(qt * qt, axis=1, keepdims=True) + 1e-06)
            qn = qt * r
            for j in range(2):
                gain = jnp.broadcast_to(q_gain[pl.ds(n * 2 + j, 1), :], (2 * hd, 2 * hd)).T
                for m in range(2):
                    gm = gain[m * hd : (m + 1) * hd, :half_rows]
                    val = (qn[j * 2 + m] * gm * hd ** (-0.5)).astype(BF16)
                    first = (n * 2 + j) * tok + m * half_rows
                    lanes = pl.ds(pl.multiple_of(first, half_rows), half_rows)
                    qtz[h, m * hd : (m + 1) * hd, lanes] = val
            return c

        lax.fori_loop(0, heads // 2, one, 0)

    def halo_copy():
        return pltpu.make_async_remote_copy(
            src_ref=halo_s,
            dst_ref=halo_r,
            send_sem=halo_sem.at[0],
            recv_sem=halo_sem.at[1],
            device_id=((sp + 1) % sp_n, tp),
            device_id_type=MESH,
        )

    def send_halo(h):
        @pl.when((sp < sp_n - 1) & (h == 1))
        def _():
            halo_copy().start()

    for copy in smalls[2:]:
        copy.wait()
    loads[0].wait()
    loads[1].wait()
    ag_mate[0].wait_recv()
    proj_kv(y)
    send_kv(y)
    loads[2].wait()
    loads[3].wait()
    proj_glu(y)
    send_halo(y)
    loads[4].wait()
    proj_q(y)
    for i in range(ag_chunks):
        ag_cross[i].wait_recv()
        ag_fwd[i].start()
    relay_kv(y)
    for i in range(ag_chunks):
        ag_fwd[i].wait_recv()
    proj_kv(yo)
    send_kv(yo)
    proj_glu(yo)
    send_halo(yo)
    proj_q(yo)

    def attend(blocks, q, diag):
        keys = jnp.concatenate(
            [kv[s, i, :half_rows, :] for s in blocks for i in range(2)], axis=0
        )
        vals = jnp.concatenate(
            [kv[s, i, half_rows:, :] for s in blocks for i in range(2)], axis=1
        )
        if diag:
            kpos = lax.broadcasted_iota(jnp.int32, (tok, tok), 0)
            qpos = lax.broadcasted_iota(jnp.int32, (tok, tok), 1)
            qpos = jnp.where(qpos >= half_rows, qpos - half_rows, qpos) + q * half_rows
            seen = kpos <= qpos
        every = dot(keys, qtz[q])
        for h in range(heads):
            sc = every[:, h * tok : (h + 1) * tok]
            if diag:
                sc = jnp.where(seen, sc, -1e30)
                top = jnp.max(sc, axis=0, keepdims=True)
                wgt = jnp.exp(sc - top)
                l_ref[h][q] = jnp.sum(wgt, axis=0, keepdims=True)
                acc[h][q] = dot(vals, wgt.astype(BF16))
            else:
                old = m_ref[h][q]
                top = jnp.maximum(old, jnp.max(sc, axis=0, keepdims=True))
                wgt = jnp.exp(sc - top)
                alpha = jnp.exp(old - top)
                l_ref[h][q] = l_ref[h][q] * alpha + jnp.sum(wgt, axis=0, keepdims=True)
                acc[h][q] = acc[h][q] * alpha + dot(vals, wgt.astype(BF16))
            m_ref[h][q] = top

    def own_block(q, c):
        attend([sp], q, True)
        return c

    lax.fori_loop(0, 2, own_block, 0)

    @pl.when(sp > 0)
    def _():
        halo_copy().wait_recv()
        gat[:HALO, :] = halo_r[...].astype(F32)

    @pl.when(sp == 0)
    def _():
        gat[:HALO, :] = jnp.zeros((HALO, chans), F32)

    st[...] = jnp.zeros_like(st)
    step_rows = 64

    def conv_cols(cc, c):
        cols = pl.ds(pl.multiple_of(cc * 128, 128), 128)
        for r0 in range(0, tok, step_rows):
            total = jnp.zeros((step_rows, 128), F32)
            for j in range(KW):
                total = total + taps[j : j + 1, cols] * gat[r0 + HALO - KW + 1 + j : r0 + HALO - KW + 1 + j + step_rows, cols]
            conv[r0 : r0 + step_rows, cols] = total
            st[0, r0 : r0 + step_rows, :] += total
            st[1, r0 : r0 + step_rows, :] += total * total
        return c

    lax.fori_loop(0, chans // 128, conv_cols, 0)
    stat[tp] = jnp.concatenate(
        [jnp.sum(st[i].T, axis=0, keepdims=True) for i in range(2)], axis=0
    )

    def stat_copy(i):
        return pltpu.make_async_remote_copy(
            src_ref=stat.at[tp],
            dst_ref=stat.at[tp],
            send_sem=stat_send.at[i],
            recv_sem=stat_recv.at[i],
            device_id=(sp, (tp + i) % tp_n),
            device_id_type=MESH,
        )

    for i in range(1, tp_n):
        stat_copy(i).start()
    relay_kv(yo)

    @pl.when(lane == 1)
    def _():
        arrived(sp - 1, y)
        arrived(sp - 1, yo)

        def partner_block(q, c):
            attend([sp - 1], q, False)
            return c

        lax.fori_loop(0, 2, partner_block, 0)

    for i in range(1, tp_n):
        stat_copy(i).wait_recv()
    sums = stat[0]
    for i in range(1, tp_n):
        sums = sums + stat[i]
    sums = sums / (chans * tp_n)
    mu = sums[0:1]
    inv = lax.rsqrt(sums[1:2] - mu * mu + 1e-05)
    mu_t = jnp.broadcast_to(mu, (128, tok)).T
    inv_t = jnp.broadcast_to(inv, (128, tok)).T
    for cc in range(0, chans, 128):
        val = (conv[:, cc : cc + 128] - mu_t) * inv_t * ln_gain[:, cc : cc + 128]
        c_out[:, cc : cc + 128] = (val * jax.nn.sigmoid(val)).astype(BF16)
    loads[5].wait()
    wide = y_s.shape[2]
    chunks = width // wide

    def out_conv(n, c):
        cols = pl.ds(pl.multiple_of(n * wide, wide), wide)
        part[:, cols] = dot(c_out[...], woc[:, cols])
        return c

    lax.fori_loop(0, chunks, out_conv, 0)

    def pairs(q, first):
        def one(i, c):
            p = pos - 1 - i
            if first:
                arrived(p * 2 + 1 - lane, y)
                arrived(p * 2 + 1 - lane, yo)
            attend([p * 2, p * 2 + 1], q, False)
            return c

        lax.fori_loop(0, pos, one, 0)

    sub_t = jnp.broadcast_to(sub_gain[...], (half_rows, vdim)).T

    def close_heads(q):
        at = pl.ds(pl.multiple_of(q * half_rows, half_rows), half_rows)
        for h in range(heads):
            total = l_ref[h][q]
            log_row = m_ref[h][q] + jnp.log(total)
            maps = acc[h][q] / total
            for m in range(2):
                logs[m, h : h + 1, at] = log_row[:, m * half_rows : (m + 1) * half_rows]
            diff = maps[:, :half_rows] - lam[h] * maps[:, half_rows:]
            out = diff * lax.rsqrt(jnp.mean(diff * diff, axis=0, keepdims=True) + 1e-06) * sub_t
            a_out[at, h * vdim : (h + 1) * vdim] = out.T.astype(BF16)

    loads[6].wait()

    def mate_copy(k, n):
        return pltpu.make_async_remote_copy(
            src_ref=mate_s.at[k, n],
            dst_ref=mate_r.at[k, n],
            send_sem=mate_send.at[k, n],
            recv_sem=mate_recv.at[k, n],
            device_id=(sp, mate),
            device_id_type=MESH,
        )

    def y_copy(n):
        return pltpu.make_async_remote_copy(
            src_ref=y_s.at[n],
            dst_ref=y_r.at[n],
            send_sem=y_send.at[n],
            recv_sem=y_recv.at[n],
            device_id=(sp, cross),
            device_id_type=MESH,
        )

    def half_of(h):
        return pl.ds(pl.multiple_of(h * half_rows, half_rows), half_rows)

    def owner_rows(h, c):
        return pl.ds(pl.multiple_of((h * 2 + c) * rows, rows), rows)

    def out_attn(k, h):
        def one(n, c):
            cols = pl.ds(pl.multiple_of(n * wide, wide), wide)
            part[half_of(h), cols] += dot(a_out[half_of(h), :], woa[:, cols])
            mate_s[k, n] = part[owner_rows(h, 1 - core), cols].astype(BF16)
            mate_copy(k, n).start()
            return c

        lax.fori_loop(0, chunks, one, 0)

    pairs(yo, True)
    close_heads(yo)
    out_attn(0, yo)

    def forward(n, c):
        cols = pl.ds(pl.multiple_of(n * wide, wide), wide)
        mate_copy(0, n).wait_recv()
        y_s[n] = (part[owner_rows(yo, core), cols] + mate_r[0, n].astype(F32)).astype(BF16)
        y_copy(n).start()
        return c

    lax.fori_loop(0, chunks, forward, 0)
    pairs(y, False)
    close_heads(y)
    out_attn(1, y)

    def finish(n, c):
        cols = pl.ds(pl.multiple_of(n * wide, wide), wide)
        mate_copy(1, n).wait_recv()
        y_copy(n).wait_recv()
        total = part[owner_rows(y, core), cols] + mate_r[1, n].astype(F32) + y_r[n].astype(F32)
        mixed[:, cols] = total.astype(BF16)
        return c

    lax.fori_loop(0, chunks, finish, 0)

    for copy in ag_cross + ag_mate + ag_fwd:
        copy.wait_send()
    for i in range(1, tp_n):
        stat_copy(i).wait_send()

    @pl.when(sp < sp_n - 1)
    def _():
        halo_copy().wait_send()

    for h in range(2):

        @pl.when(lane == 0)
        def _():
            x_copy(pos, h).wait_send()

        def z_done(i, c):
            z_copy(npos - 1 - i, h).wait_send()
            return c

        lax.fori_loop(0, npos - 1 - pos, z_done, 0)

        def x_done(i, c):
            x_copy(i, h).wait_send()
            return c

        lax.fori_loop(0, pos, x_done, 0)

    def rs_done(n, c):
        mate_copy(0, n).wait_send()
        mate_copy(1, n).wait_send()
        y_copy(n).wait_send()
        return c

    lax.fori_loop(0, chunks, rs_done, 0)


def put_out(mixed, logs, mixed_hbm, logs_hbm, sem):
    copies = [
        pltpu.make_async_copy(mixed, mixed_hbm, sem.at[0]),
        pltpu.make_async_copy(logs, logs_hbm, sem.at[1]),
    ]
    for copy in copies:
        copy.start()
    for copy in copies:
        copy.wait()


def on_device(sp_n, tp_n, *args):
    (
        tokens,
        norm_gain,
        w_glu_a,
        w_glu_b,
        conv_taps,
        ln_gain,
        w_query,
        w_key,
        w_value,
        query_gain,
        key_gain,
        lam_head,
        sub_gain,
        w_out_conv,
        w_out_attn,
    ) = args
    rows, width = tokens.shape
    tok = rows * tp_n
    half = tok // 2
    chans = conv_taps.shape[1]
    heads = lam_head.shape[0]
    qcols = w_query.shape[1]
    kcols = w_key.shape[1]
    vcols = w_value.shape[1]
    vdim = sub_gain.shape[0]
    acols = w_out_attn.shape[0]
    chunks = 4
    wide = width // chunks
    vmem = pl.BlockSpec(memory_space=pltpu.VMEM)
    dma = pltpu.SemaphoreType.DMA
    hbm = pl.BlockSpec(memory_space=pltpu.HBM)
    mixed, logs = pl.pallas_call(
        functools.partial(kernel, sp_n, tp_n),
        out_shape=(
            pltpu.VMEM((rows, width), BF16),
            pltpu.VMEM((2, heads, tok), F32),
        ),
        in_specs=[hbm] * 15,
        out_specs=(vmem, vmem),
        scratch_shapes=[
            pltpu.VMEM((rows, width), BF16),
            pltpu.VMEM((1, width), F32),
            pltpu.VMEM(conv_taps.shape, F32),
            pltpu.VMEM((1, chans), F32),
            pltpu.VMEM(query_gain.shape, F32),
            pltpu.VMEM(key_gain.shape, F32),
            pltpu.SMEM((heads,), F32),
            pltpu.VMEM((1, vdim), F32),
            pltpu.VMEM((width, chans), BF16),
            pltpu.VMEM((width, chans), BF16),
            pltpu.VMEM((width, qcols), BF16),
            pltpu.VMEM((width, kcols + vcols), BF16),
            pltpu.VMEM((chans, width), BF16),
            pltpu.VMEM((acols, width), BF16),
            pltpu.VMEM((tp_n, rows, width), BF16),
            pltpu.VMEM((sp_n, 2, half + vcols, half), BF16),
            pltpu.VMEM((2, kcols, heads * tok), BF16),
            pltpu.VMEM((HALO + tok, chans), F32),
            pltpu.VMEM((HALO, chans), BF16),
            pltpu.VMEM((HALO, chans), BF16),
            pltpu.VMEM((tok, chans), F32),
            pltpu.VMEM((2, tok, 128), F32),
            pltpu.VMEM((tp_n, 2, tok), F32),
            pltpu.VMEM((tok, chans), BF16),
            [pltpu.VMEM((2, 1, tok), F32) for _ in range(heads)],
            [pltpu.VMEM((2, 1, tok), F32) for _ in range(heads)],
            [pltpu.VMEM((2, vdim, tok), F32) for _ in range(heads)],
            pltpu.VMEM((tok, acols), BF16),
            pltpu.VMEM((tok, width), F32),
            pltpu.VMEM((2, chunks, rows, wide), BF16),
            pltpu.VMEM((2, chunks, rows, wide), BF16),
            pltpu.VMEM((chunks, rows, wide), BF16),
            pltpu.VMEM((chunks, rows, wide), BF16),
            dma((8,)),
            dma((7,)),
            dma((3, 4)),
            dma((3, 4)),
            dma((sp_n // 2, 2)),
            dma((sp_n // 2, 2)),
            dma((sp_n, 2)),
            dma((2,)),
            dma((tp_n,)),
            dma((tp_n,)),
            dma((2, chunks)),
            dma((2, chunks)),
            dma((chunks,)),
            dma((chunks,)),
        ],
        compiler_params=pltpu.CompilerParams(
            collective_id=0, has_side_effects=True, vmem_limit_bytes=56 * 2**20
        ),
    )(
        tokens,
        norm_gain.reshape(1, -1),
        w_glu_a,
        w_glu_b,
        conv_taps,
        ln_gain.reshape(1, -1),
        w_query,
        w_key,
        w_value,
        query_gain,
        key_gain,
        lam_head,
        sub_gain.reshape(1, -1),
        w_out_conv,
        w_out_attn,
    )
    return pl.pallas_call(
        put_out,
        out_shape=(
            jax.ShapeDtypeStruct((rows, width), BF16),
            jax.ShapeDtypeStruct((2, heads, tok), F32),
        ),
        in_specs=[vmem, vmem],
        out_specs=(hbm, hbm),
        scratch_shapes=[dma((2,))],
    )(
        pltpu.with_memory_space_constraint(mixed, pltpu.VMEM),
        pltpu.with_memory_space_constraint(logs, pltpu.VMEM),
    )


def solution(mesh):
    return jax.shard_map(
        functools.partial(on_device, mesh.shape["sp"], mesh.shape["tp"]),
        mesh=mesh,
        in_specs=(
            P(("sp", "tp"), None),
            P(),
            P(None, "tp"),
            P(None, "tp"),
            P(None, "tp"),
            P("tp"),
            P(None, "tp"),
            P(None, "tp"),
            P(None, "tp"),
            P("tp", None),
            P("tp", None),
            P("tp"),
            P(),
            P("tp", None),
            P("tp", None),
        ),
        out_specs=(P(("sp", "tp"), None), P(None, "tp", "sp")),
        check_vma=False,
    )
```

```python
import functools

import jax
import jax.numpy as jnp
from jax import lax
from jax.experimental import pallas as pl
from jax.experimental.pallas import tpu as pltpu
from jax.sharding import PartitionSpec as P

KW = 31
HALO = 32
F32 = jnp.float32
BF16 = jnp.bfloat16
MESH = pl.DeviceIdType.MESH


def dot(a, b):
    return jnp.dot(a, b, preferred_element_type=F32)


def kernel(
    sp_n,
    tp_n,
    tokens_hbm,
    norm_gain_hbm,
    w_glu_a,
    w_glu_b,
    taps_hbm,
    ln_gain_hbm,
    w_query,
    w_key,
    w_value,
    q_gain_hbm,
    k_gain_hbm,
    lam_hbm,
    sub_gain_hbm,
    w_out_conv,
    w_out_attn,
    mixed,
    logs,
    tokens,
    norm_gain,
    taps,
    ln_gain,
    q_gain,
    k_gain,
    lam,
    sub_gain,
    wa,
    wb,
    wq,
    wkv,
    woc,
    woa,
    nrm,
    kv,
    qtz,
    gat,
    halo_s,
    halo_r,
    conv,
    st,
    stat,
    c_out,
    m_ref,
    l_ref,
    acc,
    a_out,
    part,
    mate_s,
    mate_r,
    y_s,
    y_r,
    w_sem,
    ag_send,
    ag_recv,
    z_send,
    x_send,
    kv_recv,
    halo_sem,
    stat_send,
    stat_recv,
    mate_send,
    mate_recv,
    y_send,
    y_recv,
):
    sp = lax.axis_index("sp")
    tp = lax.axis_index("tp")
    rows = tokens.shape[0]
    width = tokens.shape[1]
    tok = rows * tp_n
    half_rows = tok // 2
    heads = q_gain.shape[0]
    vdim = sub_gain.shape[1]
    hd = q_gain.shape[1] // 2
    chans = taps.shape[1]
    core = tp % 2
    y = tp // 2
    yo = 1 - y
    mate = tp + 1 - 2 * core
    cross = (tp + 2) % 4
    lane = sp % 2
    pos = sp // 2
    npos = sp_n // 2
    xmate = sp + 1 - 2 * lane

    bar = pltpu.get_barrier_semaphore()

    def greet_sp(i, c):
        pl.semaphore_signal(bar, inc=1, device_id=((sp + i) % sp_n, tp), device_id_type=MESH)
        return c

    lax.fori_loop(1, sp_n, greet_sp, 0)
    for i in range(1, tp_n):
        pl.semaphore_signal(bar, inc=1, device_id=(sp, (tp + i) % tp_n), device_id_type=MESH)

    kw = w_key.shape[1]
    loads = [
        pltpu.make_async_copy(src, dst, w_sem.at[i])
        for i, (src, dst) in enumerate(
            [
                (tokens_hbm, tokens),
                (norm_gain_hbm, norm_gain),
                (w_key, wkv.at[:, :kw]),
                (w_value, wkv.at[:, kw:]),
                (k_gain_hbm, k_gain),
                (w_glu_a, wa),
                (w_glu_b, wb),
                (q_gain_hbm, q_gain),
                (w_query, wq),
                (taps_hbm, taps),
                (ln_gain_hbm, ln_gain),
                (w_out_conv, woc),
                (sub_gain_hbm, sub_gain),
                (lam_hbm, lam),
                (w_out_attn, woa),
            ]
        )
    ]
    for copy in loads:
        copy.start()

    def loaded(lo, hi):
        for copy in loads[lo:hi]:
            copy.wait()

    qtz[...] = jnp.zeros_like(qtz)
    loaded(0, 2)
    x = tokens[...].astype(F32)
    scale = lax.rsqrt(jnp.mean(x * x, axis=-1, keepdims=True) + 1e-06)
    nrm[tp] = (x * scale * norm_gain[...]).astype(BF16)
    pl.semaphore_wait(bar, sp_n - 1 + tp_n - 1)

    ag_chunks = 4

    def ag_copy(slot, k, i, target):
        piece = pl.ds(i * (rows // ag_chunks), rows // ag_chunks)
        return pltpu.make_async_remote_copy(
            src_ref=nrm.at[slot, piece],
            dst_ref=nrm.at[slot, piece],
            send_sem=ag_send.at[k, i],
            recv_sem=ag_recv.at[k, i],
            device_id=(sp, target),
            device_id_type=MESH,
        )

    ag_cross = [ag_copy(tp, 0, i, cross) for i in range(ag_chunks)]
    ag_mate = [
        pltpu.make_async_remote_copy(
            src_ref=nrm.at[tp],
            dst_ref=nrm.at[tp],
            send_sem=ag_send.at[1, 0],
            recv_sem=ag_recv.at[1, 0],
            device_id=(sp, mate),
            device_id_type=MESH,
        )
    ]
    ag_fwd = [ag_copy(cross, 2, i, mate) for i in range(ag_chunks)]
    for copy in ag_cross + ag_mate:
        copy.start()

    def half_in(h):
        return nrm[pl.ds(2 * h, 2)].reshape(half_rows, width)

    def proj_kv(h):
        res = dot(half_in(h), wkv[...])
        k = res[:, :kw]
        v = res[:, kw:]
        first = lax.broadcasted_iota(jnp.int32, k.shape, 1) < hd
        sq = k * k
        s0 = jnp.sum(jnp.where(first, sq, 0.0), axis=1, keepdims=True)
        s1 = jnp.sum(jnp.where(first, 0.0, sq), axis=1, keepdims=True)
        r = jnp.where(first, lax.rsqrt(s0 / hd + 1e-06), lax.rsqrt(s1 / hd + 1e-06))
        kv[sp, h, :half_rows, :] = (k * r * k_gain[...]).astype(BF16)
        kv[sp, h, half_rows:, :] = v.T.astype(BF16)

    def z_copy(t, h):
        return pltpu.make_async_remote_copy(
            src_ref=kv.at[sp, h],
            dst_ref=kv.at[sp, h],
            send_sem=z_send.at[t, h],
            recv_sem=kv_recv.at[sp, h],
            device_id=(t * 2 + lane, tp),
            device_id_type=MESH,
        )

    def x_copy(p, h):
        s = p * 2 + lane
        return pltpu.make_async_remote_copy(
            src_ref=kv.at[s, h],
            dst_ref=kv.at[s, h],
            send_sem=x_send.at[p, h],
            recv_sem=kv_recv.at[s, h],
            device_id=(xmate, tp),
            device_id_type=MESH,
        )

    def arrived(s, h):
        pltpu.make_async_remote_copy(
            src_ref=kv.at[s, h],
            dst_ref=kv.at[s, h],
            send_sem=x_send.at[0, h],
            recv_sem=kv_recv.at[s, h],
            device_id=(xmate, tp),
            device_id_type=MESH,
        ).wait_recv()

    def send_kv(h):
        @pl.when(lane == 0)
        def _():
            x_copy(pos, h).start()

        def one(i, c):
            z_copy(npos - 1 - i, h).start()
            return c

        lax.fori_loop(0, npos - 1 - pos, one, 0)

    def relay_kv(h):
        def one(i, c):
            p = pos - 1 - i
            arrived(p * 2 + lane, h)
            x_copy(p, h).start()
            return c

        lax.fori_loop(0, pos, one, 0)

    def proj_glu(h):
        xin = half_in(h)
        wide = 256

        def one(n, c):
            cols = pl.ds(pl.multiple_of(n * wide, wide), wide)
            a = dot(xin, wa[:, cols])
            b = dot(xin, wb[:, cols])
            g = (a * jax.nn.sigmoid(b)).astype(BF16)
            at = pl.ds(pl.multiple_of(HALO + h * half_rows, HALO), half_rows)
            for j in range(wide // 128):
                gat[n * (wide // 128) + j, at, :] = g[:, j * 128 : (j + 1) * 128].astype(F32)

            @pl.when(h == 1)
            def _():
                halo_s[:, cols] = g[half_rows - HALO :, :]

            return c

        for n in range(chans // wide):
            one(n, 0)

    def proj_q(h):
        xin = half_in(h)

        def one(n, c):
            q = dot(xin, wq[:, pl.ds(pl.multiple_of(n * 4 * hd, 4 * hd), 4 * hd)])
            qt = q.T.reshape(4, hd, half_rows)
            r = lax.rsqrt(jnp.mean(qt * qt, axis=1, keepdims=True) + 1e-06)
            qn = qt * r
            for j in range(2):
                gain = jnp.broadcast_to(q_gain[pl.ds(n * 2 + j, 1), :], (2 * hd, 2 * hd)).T
                for m in range(2):
                    gm = gain[m * hd : (m + 1) * hd, :half_rows]
                    val = (qn[j * 2 + m] * gm * hd ** (-0.5)).astype(BF16)
                    first = (n * 2 + j) * tok + m * half_rows
                    lanes = pl.ds(pl.multiple_of(first, half_rows), half_rows)
                    qtz[h, m * hd : (m + 1) * hd, lanes] = val
            return c

        for n in range(heads // 2):
            one(n, 0)

    def halo_copy():
        return pltpu.make_async_remote_copy(
            src_ref=halo_s,
            dst_ref=halo_r,
            send_sem=halo_sem.at[0],
            recv_sem=halo_sem.at[1],
            device_id=((sp + 1) % sp_n, tp),
            device_id_type=MESH,
        )

    def send_halo(h):
        @pl.when((sp < sp_n - 1) & (h == 1))
        def _():
            halo_copy().start()

    loaded(2, 5)
    ag_mate[0].wait_recv()
    proj_kv(y)
    send_kv(y)
    loaded(5, 7)
    proj_glu(y)
    send_halo(y)
    loaded(7, 9)
    proj_q(y)
    for i in range(ag_chunks):
        ag_cross[i].wait_recv()
        ag_fwd[i].start()
    for i in range(ag_chunks):
        ag_fwd[i].wait_recv()
    proj_glu(yo)
    send_halo(yo)
    proj_kv(yo)
    send_kv(yo)
    relay_kv(y)
    proj_q(yo)

    def attend(blocks, q, diag):
        keys = jnp.concatenate(
            [kv[s, i, :half_rows, :] for s in blocks for i in range(2)], axis=0
        )
        vals = jnp.concatenate(
            [kv[s, i, half_rows:, :] for s in blocks for i in range(2)], axis=1
        )
        if diag:
            kpos = lax.broadcasted_iota(jnp.int32, (tok, tok), 0)
            qpos = lax.broadcasted_iota(jnp.int32, (tok, tok), 1)
            qpos = jnp.where(qpos >= half_rows, qpos - half_rows, qpos) + q * half_rows
            seen = kpos <= qpos
        every = dot(keys, qtz[q])
        for h in range(heads):
            sc = every[:, h * tok : (h + 1) * tok]
            if diag:
                sc = jnp.where(seen, sc, -1e30)
                top = jnp.max(sc, axis=0, keepdims=True)
                wgt = jnp.exp(sc - top)
                l_ref[h][q] = jnp.sum(wgt, axis=0, keepdims=True)
                acc[h][q] = dot(vals, wgt.astype(BF16))
            else:
                old = m_ref[h][q]
                top = jnp.maximum(old, jnp.max(sc, axis=0, keepdims=True))
                wgt = jnp.exp(sc - top)
                alpha = jnp.exp(old - top)
                l_ref[h][q] = l_ref[h][q] * alpha + jnp.sum(wgt, axis=0, keepdims=True)
                acc[h][q] = acc[h][q] * alpha + dot(vals, wgt.astype(BF16))
            m_ref[h][q] = top

    step_rows = 64
    loaded(9, 10)

    def conv_half(h):
        @pl.when((h == 0) & (sp > 0))
        def _():
            halo_copy().wait_recv()
            for j in range(chans // 128):
                gat[j, :HALO, :] = halo_r[:, j * 128 : (j + 1) * 128].astype(F32)

        @pl.when((h == 0) & (sp == 0))
        def _():
            gat[:, :HALO, :] = jnp.zeros((chans // 128, HALO, 128), F32)

        st[...] = jnp.zeros_like(st)

        def conv_cols(cc, c):
            cols = pl.ds(pl.multiple_of(cc * 128, 128), 128)
            rows_in = gat.at[cc, pl.ds(pl.multiple_of(h * half_rows, half_rows), HALO + half_rows), :]
            rows_out = conv.at[cc, pl.ds(pl.multiple_of(h * half_rows, half_rows), half_rows), :]
            for r0 in range(0, half_rows, step_rows):
                total = jnp.zeros((step_rows, 128), F32)
                for j in range(KW):
                    first = r0 + HALO - KW + 1 + j
                    total = total + taps[j : j + 1, cols] * rows_in[first : first + step_rows, :]
                rows_out[r0 : r0 + step_rows, :] = total
                st[0, r0 : r0 + step_rows, :] += total
                st[1, r0 : r0 + step_rows, :] += total * total
            return c

        lax.fori_loop(0, chans // 128, conv_cols, 0)
        stat[h, tp] = jnp.concatenate(
            [jnp.sum(st[i].T, axis=0, keepdims=True) for i in range(2)], axis=0
        )
        for i in range(1, tp_n):
            stat_copy(h, i).start()

    def stat_copy(h, i):
        return pltpu.make_async_remote_copy(
            src_ref=stat.at[h, tp],
            dst_ref=stat.at[h, tp],
            send_sem=stat_send.at[h, i],
            recv_sem=stat_recv.at[h, i],
            device_id=(sp, (tp + i) % tp_n),
            device_id_type=MESH,
        )

    wide = y_s.shape[2]
    chunks = width // wide

    def half_of(h):
        return pl.ds(pl.multiple_of(h * half_rows, half_rows), half_rows)

    def close_conv(h):
        for i in range(1, tp_n):
            stat_copy(h, i).wait_recv()
        sums = stat[h, 0]
        for i in range(1, tp_n):
            sums = sums + stat[h, i]
        sums = sums / (chans * tp_n)
        mu = sums[0:1]
        inv = lax.rsqrt(sums[1:2] - mu * mu + 1e-05)
        mu_t = jnp.broadcast_to(mu, (128, half_rows)).T
        inv_t = jnp.broadcast_to(inv, (128, half_rows)).T
        for cc in range(chans // 128):
            cols = slice(cc * 128, (cc + 1) * 128)
            val = (conv[cc, half_of(h), :] - mu_t) * inv_t * ln_gain[:, cols]
            c_out[half_of(h), cols] = (val * jax.nn.sigmoid(val)).astype(BF16)

    def out_conv(h):
        for n in range(chunks):
            cols = slice(n * wide, (n + 1) * wide)
            part[half_of(h), cols] = dot(c_out[half_of(h), :], woc[:, cols])

    conv_half(yo)
    attend([sp], yo, True)
    conv_half(y)
    attend([sp], y, True)
    loaded(10, 11)
    close_conv(yo)
    loaded(11, 12)
    out_conv(yo)
    relay_kv(yo)

    @pl.when(lane == 1)
    def _():
        arrived(sp - 1, y)
        arrived(sp - 1, yo)
        attend([sp - 1], yo, False)
        attend([sp - 1], y, False)

    close_conv(y)
    out_conv(y)

    def pairs(q, first):
        def one(i, c):
            p = pos - 1 - i
            if first:
                arrived(p * 2 + 1 - lane, y)
                arrived(p * 2 + 1 - lane, yo)
            attend([p * 2, p * 2 + 1], q, False)
            return c

        lax.fori_loop(0, pos, one, 0)

    loaded(12, 15)
    sub_t = jnp.broadcast_to(sub_gain[...], (half_rows, vdim)).T

    def close_heads(q):
        at = pl.ds(pl.multiple_of(q * half_rows, half_rows), half_rows)
        for h in range(heads):
            total = l_ref[h][q]
            log_row = m_ref[h][q] + jnp.log(total)
            maps = acc[h][q] / total
            for m in range(2):
                logs[m, h : h + 1, at] = log_row[:, m * half_rows : (m + 1) * half_rows]
            diff = maps[:, :half_rows] - lam[h] * maps[:, half_rows:]
            out = diff * lax.rsqrt(jnp.mean(diff * diff, axis=0, keepdims=True) + 1e-06) * sub_t
            a_out[at, h * vdim : (h + 1) * vdim] = out.T.astype(BF16)

    def mate_copy(k, n):
        return pltpu.make_async_remote_copy(
            src_ref=mate_s.at[k, n],
            dst_ref=mate_r.at[k, n],
            send_sem=mate_send.at[k, n],
            recv_sem=mate_recv.at[k, n],
            device_id=(sp, mate),
            device_id_type=MESH,
        )

    def y_copy(n):
        return pltpu.make_async_remote_copy(
            src_ref=y_s.at[n],
            dst_ref=y_r.at[n],
            send_sem=y_send.at[n],
            recv_sem=y_recv.at[n],
            device_id=(sp, cross),
            device_id_type=MESH,
        )

    def owner_rows(h, c):
        return pl.ds(pl.multiple_of((h * 2 + c) * rows, rows), rows)

    def out_attn(k, h):
        for piece in (range(0, 1), range(1, chunks)):
            for n in piece:
                cols = slice(n * wide, (n + 1) * wide)
                part[half_of(h), cols] += dot(a_out[half_of(h), :], woa[:, cols])
            for n in piece:
                cols = slice(n * wide, (n + 1) * wide)
                mate_s[k, n] = part[owner_rows(h, 1 - core), cols].astype(BF16)
                mate_copy(k, n).start()

    pairs(yo, True)
    close_heads(yo)
    out_attn(0, yo)

    def forward(n, c):
        cols = pl.ds(pl.multiple_of(n * wide, wide), wide)
        mate_copy(0, n).wait_recv()
        y_s[n] = (part[owner_rows(yo, core), cols] + mate_r[0, n].astype(F32)).astype(BF16)
        y_copy(n).start()
        return c

    lax.fori_loop(0, chunks, forward, 0)
    pairs(y, False)
    close_heads(y)
    out_attn(1, y)

    def finish(n, c):
        cols = pl.ds(pl.multiple_of(n * wide, wide), wide)
        mate_copy(1, n).wait_recv()
        y_copy(n).wait_recv()
        total = part[owner_rows(y, core), cols] + mate_r[1, n].astype(F32) + y_r[n].astype(F32)
        mixed[:, cols] = total.astype(BF16)
        return c

    lax.fori_loop(0, chunks, finish, 0)

    for copy in ag_cross + ag_mate + ag_fwd:
        copy.wait_send()
    for h in range(2):
        for i in range(1, tp_n):
            stat_copy(h, i).wait_send()

    @pl.when(sp < sp_n - 1)
    def _():
        halo_copy().wait_send()

    for h in range(2):

        @pl.when(lane == 0)
        def _():
            x_copy(pos, h).wait_send()

        def z_done(i, c):
            z_copy(npos - 1 - i, h).wait_send()
            return c

        lax.fori_loop(0, npos - 1 - pos, z_done, 0)

        def x_done(i, c):
            x_copy(i, h).wait_send()
            return c

        lax.fori_loop(0, pos, x_done, 0)

    def rs_done(n, c):
        mate_copy(0, n).wait_send()
        mate_copy(1, n).wait_send()
        y_copy(n).wait_send()
        return c

    lax.fori_loop(0, chunks, rs_done, 0)


def put_out(mixed, logs, mixed_hbm, logs_hbm, sem):
    copies = [
        pltpu.make_async_copy(mixed, mixed_hbm, sem.at[0]),
        pltpu.make_async_copy(logs, logs_hbm, sem.at[1]),
    ]
    for copy in copies:
        copy.start()
    for copy in copies:
        copy.wait()


def on_device(sp_n, tp_n, *args):
    (
        tokens,
        norm_gain,
        w_glu_a,
        w_glu_b,
        conv_taps,
        ln_gain,
        w_query,
        w_key,
        w_value,
        query_gain,
        key_gain,
        lam_head,
        sub_gain,
        w_out_conv,
        w_out_attn,
    ) = args
    rows, width = tokens.shape
    tok = rows * tp_n
    half = tok // 2
    chans = conv_taps.shape[1]
    heads = lam_head.shape[0]
    qcols = w_query.shape[1]
    kcols = w_key.shape[1]
    vcols = w_value.shape[1]
    vdim = sub_gain.shape[0]
    acols = w_out_attn.shape[0]
    chunks = 4
    wide = width // chunks
    vmem = pl.BlockSpec(memory_space=pltpu.VMEM)
    dma = pltpu.SemaphoreType.DMA
    hbm = pl.BlockSpec(memory_space=pltpu.HBM)
    mixed, logs = pl.pallas_call(
        functools.partial(kernel, sp_n, tp_n),
        out_shape=(
            pltpu.VMEM((rows, width), BF16),
            pltpu.VMEM((2, heads, tok), F32),
        ),
        in_specs=[hbm] * 15,
        out_specs=(vmem, vmem),
        scratch_shapes=[
            pltpu.VMEM((rows, width), BF16),
            pltpu.VMEM((1, width), F32),
            pltpu.VMEM(conv_taps.shape, F32),
            pltpu.VMEM((1, chans), F32),
            pltpu.VMEM(query_gain.shape, F32),
            pltpu.VMEM(key_gain.shape, F32),
            pltpu.SMEM((heads,), F32),
            pltpu.VMEM((1, vdim), F32),
            pltpu.VMEM((width, chans), BF16),
            pltpu.VMEM((width, chans), BF16),
            pltpu.VMEM((width, qcols), BF16),
            pltpu.VMEM((width, kcols + vcols), BF16),
            pltpu.VMEM((chans, width), BF16),
            pltpu.VMEM((acols, width), BF16),
            pltpu.VMEM((tp_n, rows, width), BF16),
            pltpu.VMEM((sp_n, 2, half + vcols, half), BF16),
            pltpu.VMEM((2, kcols, heads * tok), BF16),
            pltpu.VMEM((chans // 128, HALO + tok, 128), F32),
            pltpu.VMEM((HALO, chans), BF16),
            pltpu.VMEM((HALO, chans), BF16),
            pltpu.VMEM((chans // 128, tok, 128), F32),
            pltpu.VMEM((2, half, 128), F32),
            pltpu.VMEM((2, tp_n, 2, half), F32),
            pltpu.VMEM((tok, chans), BF16),
            [pltpu.VMEM((2, 1, tok), F32) for _ in range(heads)],
            [pltpu.VMEM((2, 1, tok), F32) for _ in range(heads)],
            [pltpu.VMEM((2, vdim, tok), F32) for _ in range(heads)],
            pltpu.VMEM((tok, acols), BF16),
            pltpu.VMEM((tok, width), F32),
            pltpu.VMEM((2, chunks, rows, wide), BF16),
            pltpu.VMEM((2, chunks, rows, wide), BF16),
            pltpu.VMEM((chunks, rows, wide), BF16),
            pltpu.VMEM((chunks, rows, wide), BF16),
            dma((15,)),
            dma((3, 4)),
            dma((3, 4)),
            dma((sp_n // 2, 2)),
            dma((sp_n // 2, 2)),
            dma((sp_n, 2)),
            dma((2,)),
            dma((2, tp_n)),
            dma((2, tp_n)),
            dma((2, chunks)),
            dma((2, chunks)),
            dma((chunks,)),
            dma((chunks,)),
        ],
        compiler_params=pltpu.CompilerParams(
            collective_id=0, has_side_effects=True, vmem_limit_bytes=56 * 2**20
        ),
    )(
        tokens,
        norm_gain.reshape(1, -1),
        w_glu_a,
        w_glu_b,
        conv_taps,
        ln_gain.reshape(1, -1),
        w_query,
        w_key,
        w_value,
        query_gain,
        key_gain,
        lam_head,
        sub_gain.reshape(1, -1),
        w_out_conv,
        w_out_attn,
    )
    return pl.pallas_call(
        put_out,
        out_shape=(
            jax.ShapeDtypeStruct((rows, width), BF16),
            jax.ShapeDtypeStruct((2, heads, tok), F32),
        ),
        in_specs=[vmem, vmem],
        out_specs=(hbm, hbm),
        scratch_shapes=[dma((2,))],
    )(
        pltpu.with_memory_space_constraint(mixed, pltpu.VMEM),
        pltpu.with_memory_space_constraint(logs, pltpu.VMEM),
    )


def solution(mesh):
    return jax.shard_map(
        functools.partial(on_device, mesh.shape["sp"], mesh.shape["tp"]),
        mesh=mesh,
        in_specs=(
            P(("sp", "tp"), None),
            P(),
            P(None, "tp"),
            P(None, "tp"),
            P(None, "tp"),
            P("tp"),
            P(None, "tp"),
            P(None, "tp"),
            P(None, "tp"),
            P("tp", None),
            P("tp", None),
            P("tp"),
            P(),
            P("tp", None),
            P("tp", None),
        ),
        out_specs=(P(("sp", "tp"), None), P(None, "tp", "sp")),
        check_vma=False,
    )
```

```python
import functools

import jax
import jax.numpy as jnp
from jax import lax
from jax.experimental import pallas as pl
from jax.experimental.pallas import tpu as pltpu
from jax.sharding import PartitionSpec as P

KW = 31
HALO = 32
LOG2_E = 1.4426950408889634
LN_2 = 0.6931471805599453
F32 = jnp.float32
BF16 = jnp.bfloat16
MESH = pl.DeviceIdType.MESH


def dot(a, b):
    return jnp.dot(a, b, preferred_element_type=F32)


def kernel(
    sp_n,
    tp_n,
    tokens_hbm,
    norm_gain_hbm,
    w_glu_a,
    w_glu_b,
    taps_hbm,
    ln_gain_hbm,
    w_query,
    w_key,
    w_value,
    q_gain_hbm,
    k_gain_hbm,
    lam_hbm,
    sub_gain_hbm,
    w_out_conv,
    w_out_attn,
    mixed,
    logs,
    tokens,
    norm_gain,
    taps,
    ln_gain,
    q_gain,
    k_gain,
    lam,
    sub_gain,
    wa,
    wb,
    wq,
    wkv,
    woc,
    woa,
    nrm,
    kv,
    qtz,
    gat,
    halo_s,
    halo_r,
    conv,
    st,
    stat,
    c_out,
    m_ref,
    l_ref,
    acc,
    a_out,
    part,
    mate_s,
    mate_r,
    y_s,
    y_r,
    w_sem,
    ag_send,
    ag_recv,
    z_send,
    x_send,
    kv_recv,
    halo_sem,
    stat_send,
    stat_recv,
    mate_send,
    mate_recv,
    y_send,
    y_recv,
):
    sp = lax.axis_index("sp")
    tp = lax.axis_index("tp")
    rows = tokens.shape[0]
    width = tokens.shape[1]
    tok = rows * tp_n
    half_rows = tok // 2
    heads = q_gain.shape[0]
    vdim = sub_gain.shape[1]
    hd = q_gain.shape[1] // 2
    chans = taps.shape[1]
    core = tp % 2
    y = tp // 2
    yo = 1 - y
    mate = tp + 1 - 2 * core
    cross = (tp + 2) % 4
    lane = sp % 2
    pos = sp // 2
    npos = sp_n // 2
    xmate = sp + 1 - 2 * lane

    bar = pltpu.get_barrier_semaphore()

    def greet_sp(i, c):
        pl.semaphore_signal(bar, inc=1, device_id=((sp + i) % sp_n, tp), device_id_type=MESH)
        return c

    lax.fori_loop(1, sp_n, greet_sp, 0)
    for i in range(1, tp_n):
        pl.semaphore_signal(bar, inc=1, device_id=(sp, (tp + i) % tp_n), device_id_type=MESH)

    kw = w_key.shape[1]
    loads = [
        pltpu.make_async_copy(src, dst, w_sem.at[i])
        for i, (src, dst) in enumerate(
            [
                (tokens_hbm, tokens),
                (norm_gain_hbm, norm_gain),
                (w_key, wkv.at[:, :kw]),
                (w_value, wkv.at[:, kw:]),
                (k_gain_hbm, k_gain),
                (w_glu_a, wa),
                (w_glu_b, wb),
                (q_gain_hbm, q_gain),
                (w_query, wq),
                (taps_hbm, taps),
                (ln_gain_hbm, ln_gain),
                (w_out_conv, woc),
                (sub_gain_hbm, sub_gain),
                (lam_hbm, lam),
                (w_out_attn, woa),
            ]
        )
    ]
    for copy in loads:
        copy.start()

    def loaded(lo, hi):
        for copy in loads[lo:hi]:
            copy.wait()

    qtz[...] = jnp.zeros_like(qtz)
    loaded(0, 2)
    x = tokens[...].astype(F32)
    scale = lax.rsqrt(jnp.mean(x * x, axis=-1, keepdims=True) + 1e-06)
    nrm[tp] = (x * scale * norm_gain[...]).astype(BF16)
    pl.semaphore_wait(bar, sp_n - 1 + tp_n - 1)

    ag_chunks = 4

    def ag_copy(slot, k, i, target):
        piece = pl.ds((ag_chunks - 1 - i) * (rows // ag_chunks), rows // ag_chunks)
        return pltpu.make_async_remote_copy(
            src_ref=nrm.at[slot, piece],
            dst_ref=nrm.at[slot, piece],
            send_sem=ag_send.at[k, i],
            recv_sem=ag_recv.at[k, i],
            device_id=(sp, target),
            device_id_type=MESH,
        )

    ag_cross = [ag_copy(tp, 0, i, cross) for i in range(ag_chunks)]
    ag_mate = [
        pltpu.make_async_remote_copy(
            src_ref=nrm.at[tp],
            dst_ref=nrm.at[tp],
            send_sem=ag_send.at[1, 0],
            recv_sem=ag_recv.at[1, 0],
            device_id=(sp, mate),
            device_id_type=MESH,
        )
    ]
    ag_fwd = [ag_copy(cross, 2, i, mate) for i in range(ag_chunks)]
    for copy in ag_cross + ag_mate:
        copy.start()

    def half_in(h):
        return nrm[pl.ds(2 * h, 2)].reshape(half_rows, width)

    def norm_kv(xin):
        res = dot(xin, wkv[...])
        k = res[:, :kw]
        first = lax.broadcasted_iota(jnp.int32, k.shape, 1) < hd
        sq = k * k
        s0 = jnp.sum(jnp.where(first, sq, 0.0), axis=1, keepdims=True)
        s1 = jnp.sum(jnp.where(first, 0.0, sq), axis=1, keepdims=True)
        r = jnp.where(first, lax.rsqrt(s0 / hd + 1e-06), lax.rsqrt(s1 / hd + 1e-06))
        return (k * r * k_gain[...]).astype(BF16), res[:, kw:].astype(BF16)

    half_slot = rows // 2

    def first_row(i):
        return (1 - i) * half_slot

    def unit_in(i):
        at = slice(first_row(i), first_row(i) + half_slot)
        return jnp.concatenate([nrm[2 * yo, at, :], nrm[2 * yo + 1, at, :]], axis=0)

    def proj_kv_near():
        k, v = norm_kv(half_in(y))
        for i in range(2):
            for j in range(2):
                src = slice(j * rows + first_row(i), j * rows + first_row(i) + half_slot)
                dst = slice(j * half_slot, (j + 1) * half_slot)
                kv[sp, 2 * y + i, dst, :] = k[src]
                kv[sp, 2 * y + i, rows + j * half_slot : rows + (j + 1) * half_slot, :] = v[src]

    def proj_kv_far(i):
        k, v = norm_kv(unit_in(i))
        kv[sp, 2 * yo + i, :rows, :] = k
        kv[sp, 2 * yo + i, rows:, :] = v

    def kv_part(s, m):
        if m == 0:
            return kv.at[s, pl.ds(2 * y, 2)]
        return kv.at[s, pl.ds(2 * yo + m - 1, 1)]

    def z_copy(p, m, d):
        s = p * 2 + lane
        return pltpu.make_async_remote_copy(
            src_ref=kv_part(s, m),
            dst_ref=kv_part(s, m),
            send_sem=z_send.at[p, m, d - 1],
            recv_sem=kv_recv.at[s, m],
            device_id=((pos + d) * 2 + lane, tp),
            device_id_type=MESH,
        )

    last = pos == npos - 1

    def x_copy(p, m):
        s = p * 2 + lane
        return pltpu.make_async_remote_copy(
            src_ref=kv_part(s, m),
            dst_ref=kv_part(s, m),
            send_sem=x_send.at[p, m],
            recv_sem=kv_recv.at[s, m],
            device_id=(xmate, tp),
            device_id_type=MESH,
        )

    def arrived(s, m):
        pltpu.make_async_remote_copy(
            src_ref=kv_part(s, m),
            dst_ref=kv_part(s, m),
            send_sem=x_send.at[0, m],
            recv_sem=kv_recv.at[s, m],
            device_id=(xmate, tp),
            device_id_type=MESH,
        ).wait_recv()

    late = 2

    def direct_kv(then):
        def one(i, c):
            then(z_copy(pos, late, npos - 1 - pos - i))
            return c

        lax.fori_loop(0, npos - 1 - pos, one, 0)

    def tree_kv(p, m, then):
        @pl.when((p == pos) & (pos + 2 < npos))
        def _():
            then(z_copy(p, m, 2))

        @pl.when((p != pos - 1) & (pos + 1 < npos))
        def _():
            then(z_copy(p, m, 1))

    def send_kv(m):
        if m == late:
            direct_kv(lambda copy: copy.start())
        else:
            tree_kv(pos, m, lambda copy: copy.start())

        @pl.when(lane == 0)
        def _():
            x_copy(pos, m).start()

    def relay_kv(m, lo, hi=None):
        def one(i, c):
            p = pos - 1 - i
            arrived(p * 2 + lane, m)
            if m != late:
                tree_kv(p, m, lambda copy: copy.start())
            x_copy(p, m).start()
            return c

        lax.fori_loop(lo, pos if hi is None else jnp.minimum(pos, hi), one, 0)

    def relay_last(m, lo, hi):
        relay_kv(m, lo, jnp.where(last, hi, 0))

    def relay_rest(m, lo, hi):
        relay_kv(m, lo, jnp.where(last, 0, hi))

    def gate(xin, n):
        wide = 256
        cols = slice(n * wide, (n + 1) * wide)
        a = dot(xin, wa[:, cols])
        b = dot(xin, wb[:, cols])
        return (a * jax.nn.sigmoid(b)).astype(BF16)

    def proj_glu_near():
        xin = half_in(y)
        at = pl.ds(pl.multiple_of(HALO + y * half_rows, HALO), half_rows)
        for n in range(chans // 256):
            g = gate(xin, n)
            for j in range(2):
                gat[2 * n + j, at, :] = g[:, j * 128 : (j + 1) * 128].astype(F32)

            @pl.when(y == 1)
            def _():
                halo_s[:, n * 256 : (n + 1) * 256] = g[half_rows - HALO :, :]

    def proj_glu_far(i):
        xin = unit_in(i)
        for n in range(chans // 256):
            g = gate(xin, n)
            for t in range(2):
                at = pl.ds(pl.multiple_of(HALO + yo * half_rows + t * rows + first_row(i), HALO), half_slot)
                part_g = g[t * half_slot : (t + 1) * half_slot]
                for j in range(2):
                    gat[2 * n + j, at, :] = part_g[:, j * 128 : (j + 1) * 128].astype(F32)
            if i == 0:

                @pl.when(yo == 1)
                def _():
                    halo_s[:, n * 256 : (n + 1) * 256] = g[rows - HALO : rows, :]

    def proj_q(h):
        xin = half_in(h)

        def one(n, c):
            q = dot(xin, wq[:, pl.ds(pl.multiple_of(n * 4 * hd, 4 * hd), 4 * hd)])
            qt = q.T.reshape(4, hd, half_rows)
            r = lax.rsqrt(jnp.mean(qt * qt, axis=1, keepdims=True) + 1e-06)
            qn = qt * r
            for j in range(2):
                gain = jnp.broadcast_to(q_gain[pl.ds(n * 2 + j, 1), :], (2 * hd, 2 * hd)).T
                for m in range(2):
                    gm = gain[m * hd : (m + 1) * hd, :half_rows]
                    val = (qn[j * 2 + m] * gm).astype(BF16).astype(F32) * (hd ** (-0.5) * LOG2_E)
                    high = val.astype(BF16)
                    low = (val - high.astype(F32)).astype(BF16)
                    first = (n * 2 + j) * tok + m * half_rows
                    lanes = pl.ds(pl.multiple_of(first, half_rows), half_rows)
                    qtz[h, m * hd : (m + 1) * hd, lanes] = high
                    qtz[h, (m + 2) * hd : (m + 3) * hd, lanes] = low
            return c

        for n in range(heads // 2):
            one(n, 0)

    def halo_copy():
        return pltpu.make_async_remote_copy(
            src_ref=halo_s,
            dst_ref=halo_r,
            send_sem=halo_sem.at[0],
            recv_sem=halo_sem.at[1],
            device_id=((sp + 1) % sp_n, tp),
            device_id_type=MESH,
        )

    def send_halo(h):
        @pl.when((sp < sp_n - 1) & (h == 1))
        def _():
            halo_copy().start()

    loaded(2, 5)
    ag_mate[0].wait_recv()
    proj_kv_near()
    send_kv(0)
    loaded(5, 7)
    proj_glu_near()
    send_halo(y)
    loaded(7, 9)
    proj_q(y)

    def far_row(n):
        ag_cross[n].wait_recv()
        ag_fwd[n].start()

    far_row(0)
    far_row(1)
    ag_fwd[0].wait_recv()
    ag_fwd[1].wait_recv()
    proj_kv_far(0)
    send_kv(1)
    far_row(2)

    @pl.when(core == 1)
    def _():
        far_row(3)

    proj_glu_far(0)
    send_halo(yo)
    @pl.when(core == 0)
    def _():
        far_row(3)

    relay_rest(0, 0, npos)
    relay_last(0, 0, 2)
    ag_fwd[2].wait_recv()
    ag_fwd[3].wait_recv()
    proj_kv_far(1)
    send_kv(2)
    proj_glu_far(1)
    def attend(blocks, q, diag, units=(0, 1, 2, 3)):
        keys = jnp.concatenate([kv[s, u, :rows, :] for s in blocks for u in units], axis=0)
        vals = jnp.concatenate([kv[s, u, rows:, :] for s in blocks for u in units], axis=0).T
        if diag:
            e = lax.broadcasted_iota(jnp.int32, (tok, 1), 0)
            kpos = e // half_rows * half_rows + e // half_slot % 2 * rows
            kpos = kpos + (1 - e // rows % 2) * half_slot + e % half_slot
            qpos = lax.broadcasted_iota(jnp.int32, (1, tok), 1)
            qpos = jnp.where(qpos >= half_rows, qpos - half_rows, qpos) + q * half_rows
            seen = kpos <= qpos
        every = dot(jnp.concatenate([keys, keys], axis=1), qtz[q])
        for h in range(heads):
            sc = every[:, h * tok : (h + 1) * tok]
            if diag:
                sc = jnp.where(seen, sc, -1e30)
                top = jnp.max(sc, axis=0, keepdims=True)
                wgt = jnp.exp2(sc - top)
                l_ref[h][q] = jnp.sum(wgt, axis=0, keepdims=True)
                acc[h][q] = dot(vals, wgt.astype(BF16))
            else:
                old = m_ref[h][q]
                top = jnp.maximum(old, jnp.max(sc, axis=0, keepdims=True))
                wgt = jnp.exp2(sc - top)
                alpha = jnp.exp2(old - top)
                l_ref[h][q] = l_ref[h][q] * alpha + jnp.sum(wgt, axis=0, keepdims=True)
                acc[h][q] = acc[h][q] * alpha + dot(vals, wgt.astype(BF16))
            m_ref[h][q] = top

    step_rows = 64
    loaded(9, 10)

    def conv_half(h):
        @pl.when((h == 0) & (sp > 0))
        def _():
            halo_copy().wait_recv()
            for j in range(chans // 128):
                gat[j, :HALO, :] = halo_r[:, j * 128 : (j + 1) * 128].astype(F32)

        @pl.when((h == 0) & (sp == 0))
        def _():
            gat[:, :HALO, :] = jnp.zeros((chans // 128, HALO, 128), F32)

        st[...] = jnp.zeros_like(st)

        def conv_cols(cc, c):
            cols = pl.ds(pl.multiple_of(cc * 128, 128), 128)
            rows_in = gat.at[cc, pl.ds(pl.multiple_of(h * half_rows, half_rows), HALO + half_rows), :]
            rows_out = conv.at[cc, pl.ds(pl.multiple_of(h * half_rows, half_rows), half_rows), :]
            for r0 in range(0, half_rows, step_rows):
                total = jnp.zeros((step_rows, 128), F32)
                for j in range(KW):
                    first = r0 + HALO - KW + 1 + j
                    total = total + taps[j : j + 1, cols] * rows_in[first : first + step_rows, :]
                rows_out[r0 : r0 + step_rows, :] = total
                st[0, r0 : r0 + step_rows, :] += total
                st[1, r0 : r0 + step_rows, :] += total * total
            return c

        lax.fori_loop(0, chans // 128, conv_cols, 0)
        stat[h, tp] = jnp.concatenate(
            [jnp.sum(st[i].T, axis=0, keepdims=True) for i in range(2)], axis=0
        )
        for i in range(1, tp_n):
            stat_copy(h, i).start()

    def stat_copy(h, i):
        return pltpu.make_async_remote_copy(
            src_ref=stat.at[h, tp],
            dst_ref=stat.at[h, tp],
            send_sem=stat_send.at[h, i],
            recv_sem=stat_recv.at[h, i],
            device_id=(sp, (tp + i) % tp_n),
            device_id_type=MESH,
        )

    wide = y_s.shape[2]
    chunks = width // wide

    def half_of(h):
        return pl.ds(pl.multiple_of(h * half_rows, half_rows), half_rows)

    def close_conv(h):
        for i in range(1, tp_n):
            stat_copy(h, i).wait_recv()
        sums = stat[h, 0]
        for i in range(1, tp_n):
            sums = sums + stat[h, i]
        sums = sums / (chans * tp_n)
        mu = sums[0:1]
        inv = lax.rsqrt(sums[1:2] - mu * mu + 1e-05)
        mu_t = jnp.broadcast_to(mu, (128, half_rows)).T
        inv_t = jnp.broadcast_to(inv, (128, half_rows)).T
        for cc in range(chans // 128):
            cols = slice(cc * 128, (cc + 1) * 128)
            val = (conv[cc, half_of(h), :] - mu_t) * inv_t * ln_gain[:, cols]
            c_out[half_of(h), cols] = (val * jax.nn.sigmoid(val)).astype(BF16)

    def out_conv(h):
        for n in range(chunks):
            cols = slice(n * wide, (n + 1) * wide)
            part[half_of(h), cols] = dot(c_out[half_of(h), :], woc[:, cols])

    relay_rest(1, 0, 1)
    conv_half(yo)
    relay_rest(1, 1, npos)
    relay_last(1, 0, 2)
    conv_half(y)
    proj_q(yo)
    attend([sp], yo, True)
    relay_rest(2, 0, 1)
    relay_last(0, 2, npos)

    @pl.when(lane == 1)
    def _():
        for m in range(3):
            arrived(sp - 1, m)
        attend([sp - 1], yo, False)

    relay_rest(2, 1, npos)
    relay_last(1, 2, npos)
    relay_last(2, 0, 2)
    loaded(10, 11)
    close_conv(yo)
    loaded(11, 12)
    out_conv(yo)
    relay_last(2, 2, npos)
    def near_part():
        attend([sp], y, True)
        close_conv(y)
        out_conv(y)

        @pl.when(lane == 1)
        def _():
            attend([sp - 1], y, False)

    pl.when(pos > 0)(near_part)

    def pairs_far():
        def early(i, c):
            p = pos - 1 - i
            for m in range(2):
                arrived(p * 2 + 1 - lane, m)
            attend([p * 2, p * 2 + 1], yo, False, (2 * y, 2 * y + 1, 2 * yo))
            return c

        def late(i, c):
            p = pos - 1 - i
            arrived(p * 2 + 1 - lane, 2)
            attend([p * 2, p * 2 + 1], yo, False, (2 * yo + 1,))
            return c

        lax.fori_loop(0, pos, early, 0)
        lax.fori_loop(0, pos, late, 0)

    def pairs_near():
        def one(i, c):
            p = pos - 1 - i
            attend([p * 2, p * 2 + 1], y, False)
            return c

        lax.fori_loop(0, pos, one, 0)

    loaded(12, 15)
    sub_t = jnp.broadcast_to(sub_gain[...], (half_rows, vdim)).T

    def close_heads(q):
        at = pl.ds(pl.multiple_of(q * half_rows, half_rows), half_rows)
        for h in range(heads):
            total = l_ref[h][q]
            log_row = m_ref[h][q] * LN_2 + jnp.log(total)
            maps = acc[h][q] / total
            for m in range(2):
                logs[m, h : h + 1, at] = log_row[:, m * half_rows : (m + 1) * half_rows]
            diff = maps[:, :half_rows] - lam[h] * maps[:, half_rows:]
            out = diff * lax.rsqrt(jnp.mean(diff * diff, axis=0, keepdims=True) + 1e-06) * sub_t
            a_out[at, h * vdim : (h + 1) * vdim] = out.T.astype(BF16)

    def mate_copy(k, n):
        return pltpu.make_async_remote_copy(
            src_ref=mate_s.at[k, n],
            dst_ref=mate_r.at[k, n],
            send_sem=mate_send.at[k, n],
            recv_sem=mate_recv.at[k, n],
            device_id=(sp, mate),
            device_id_type=MESH,
        )

    def y_copy(n):
        return pltpu.make_async_remote_copy(
            src_ref=y_s.at[n],
            dst_ref=y_r.at[n],
            send_sem=y_send.at[n],
            recv_sem=y_recv.at[n],
            device_id=(sp, cross),
            device_id_type=MESH,
        )

    def owner_rows(h, c):
        return pl.ds(pl.multiple_of((h * 2 + c) * rows, rows), rows)

    def out_attn(k, h):
        for piece in (range(0, 1), range(1, chunks)):
            for n in piece:
                cols = slice(n * wide, (n + 1) * wide)
                part[half_of(h), cols] += dot(a_out[half_of(h), :], woa[:, cols])
            for n in piece:
                cols = slice(n * wide, (n + 1) * wide)
                mate_s[k, n] = part[owner_rows(h, 1 - core), cols].astype(BF16)
                mate_copy(k, n).start()

    pairs_far()
    close_heads(yo)
    out_attn(0, yo)
    pl.when(pos == 0)(near_part)

    def forward(n, c):
        cols = pl.ds(pl.multiple_of(n * wide, wide), wide)
        mate_copy(0, n).wait_recv()
        y_s[n] = (part[owner_rows(yo, core), cols] + mate_r[0, n].astype(F32)).astype(BF16)
        y_copy(n).start()
        return c

    lax.fori_loop(0, chunks, forward, 0)
    pairs_near()
    close_heads(y)
    out_attn(1, y)

    def finish(n, c):
        cols = pl.ds(pl.multiple_of(n * wide, wide), wide)
        mate_copy(1, n).wait_recv()
        y_copy(n).wait_recv()
        total = part[owner_rows(y, core), cols] + mate_r[1, n].astype(F32) + y_r[n].astype(F32)
        mixed[:, cols] = total.astype(BF16)
        return c

    lax.fori_loop(0, chunks, finish, 0)

    for copy in ag_cross + ag_mate + ag_fwd:
        copy.wait_send()
    for h in range(2):
        for i in range(1, tp_n):
            stat_copy(h, i).wait_send()

    @pl.when(sp < sp_n - 1)
    def _():
        halo_copy().wait_send()

    for m in range(3):

        @pl.when(lane == 0)
        def _():
            x_copy(pos, m).wait_send()

        if m == late:
            direct_kv(lambda copy: copy.wait_send())
        else:
            tree_kv(pos, m, lambda copy: copy.wait_send())

        def relay_done(p, c):
            x_copy(p, m).wait_send()
            if m != late:
                tree_kv(p, m, lambda copy: copy.wait_send())
            return c

        lax.fori_loop(0, pos, relay_done, 0)

    def rs_done(n, c):
        mate_copy(0, n).wait_send()
        mate_copy(1, n).wait_send()
        y_copy(n).wait_send()
        return c

    lax.fori_loop(0, chunks, rs_done, 0)


def put_out(mixed, logs, mixed_hbm, logs_hbm, sem):
    copies = [
        pltpu.make_async_copy(mixed, mixed_hbm, sem.at[0]),
        pltpu.make_async_copy(logs, logs_hbm, sem.at[1]),
    ]
    for copy in copies:
        copy.start()
    for copy in copies:
        copy.wait()


def on_device(sp_n, tp_n, *args):
    (
        tokens,
        norm_gain,
        w_glu_a,
        w_glu_b,
        conv_taps,
        ln_gain,
        w_query,
        w_key,
        w_value,
        query_gain,
        key_gain,
        lam_head,
        sub_gain,
        w_out_conv,
        w_out_attn,
    ) = args
    rows, width = tokens.shape
    tok = rows * tp_n
    half = tok // 2
    chans = conv_taps.shape[1]
    heads = lam_head.shape[0]
    qcols = w_query.shape[1]
    kcols = w_key.shape[1]
    vcols = w_value.shape[1]
    vdim = sub_gain.shape[0]
    acols = w_out_attn.shape[0]
    chunks = 4
    wide = width // chunks
    vmem = pl.BlockSpec(memory_space=pltpu.VMEM)
    dma = pltpu.SemaphoreType.DMA
    hbm = pl.BlockSpec(memory_space=pltpu.HBM)
    mixed, logs = pl.pallas_call(
        functools.partial(kernel, sp_n, tp_n),
        out_shape=(
            pltpu.VMEM((rows, width), BF16),
            pltpu.VMEM((2, heads, tok), F32),
        ),
        in_specs=[hbm] * 15,
        out_specs=(vmem, vmem),
        scratch_shapes=[
            pltpu.VMEM((rows, width), BF16),
            pltpu.VMEM((1, width), F32),
            pltpu.VMEM(conv_taps.shape, F32),
            pltpu.VMEM((1, chans), F32),
            pltpu.VMEM(query_gain.shape, F32),
            pltpu.VMEM(key_gain.shape, F32),
            pltpu.SMEM((heads,), F32),
            pltpu.VMEM((1, vdim), F32),
            pltpu.VMEM((width, chans), BF16),
            pltpu.VMEM((width, chans), BF16),
            pltpu.VMEM((width, qcols), BF16),
            pltpu.VMEM((width, kcols + vcols), BF16),
            pltpu.VMEM((chans, width), BF16),
            pltpu.VMEM((acols, width), BF16),
            pltpu.VMEM((tp_n, rows, width), BF16),
            pltpu.VMEM((sp_n, 4, 2 * rows, kcols), BF16),
            pltpu.VMEM((2, 2 * kcols, heads * tok), BF16),
            pltpu.VMEM((chans // 128, HALO + tok, 128), F32),
            pltpu.VMEM((HALO, chans), BF16),
            pltpu.VMEM((HALO, chans), BF16),
            pltpu.VMEM((chans // 128, tok, 128), F32),
            pltpu.VMEM((2, half, 128), F32),
            pltpu.VMEM((2, tp_n, 2, half), F32),
            pltpu.VMEM((tok, chans), BF16),
            [pltpu.VMEM((2, 1, tok), F32) for _ in range(heads)],
            [pltpu.VMEM((2, 1, tok), F32) for _ in range(heads)],
            [pltpu.VMEM((2, vdim, tok), F32) for _ in range(heads)],
            pltpu.VMEM((tok, acols), BF16),
            pltpu.VMEM((tok, width), F32),
            pltpu.VMEM((2, chunks, rows, wide), BF16),
            pltpu.VMEM((2, chunks, rows, wide), BF16),
            pltpu.VMEM((chunks, rows, wide), BF16),
            pltpu.VMEM((chunks, rows, wide), BF16),
            dma((15,)),
            dma((3, 4)),
            dma((3, 4)),
            dma((sp_n // 2, 3, max(2, sp_n // 2 - 1))),
            dma((sp_n // 2, 3)),
            dma((sp_n, 3)),
            dma((2,)),
            dma((2, tp_n)),
            dma((2, tp_n)),
            dma((2, chunks)),
            dma((2, chunks)),
            dma((chunks,)),
            dma((chunks,)),
        ],
        compiler_params=pltpu.CompilerParams(
            collective_id=0, has_side_effects=True, vmem_limit_bytes=56 * 2**20
        ),
    )(
        tokens,
        norm_gain.reshape(1, -1),
        w_glu_a,
        w_glu_b,
        conv_taps,
        ln_gain.reshape(1, -1),
        w_query,
        w_key,
        w_value,
        query_gain,
        key_gain,
        lam_head,
        sub_gain.reshape(1, -1),
        w_out_conv,
        w_out_attn,
    )
    return pl.pallas_call(
        put_out,
        out_shape=(
            jax.ShapeDtypeStruct((rows, width), BF16),
            jax.ShapeDtypeStruct((2, heads, tok), F32),
        ),
        in_specs=[vmem, vmem],
        out_specs=(hbm, hbm),
        scratch_shapes=[dma((2,))],
    )(
        pltpu.with_memory_space_constraint(mixed, pltpu.VMEM),
        pltpu.with_memory_space_constraint(logs, pltpu.VMEM),
    )


def solution(mesh):
    return jax.shard_map(
        functools.partial(on_device, mesh.shape["sp"], mesh.shape["tp"]),
        mesh=mesh,
        in_specs=(
            P(("sp", "tp"), None),
            P(),
            P(None, "tp"),
            P(None, "tp"),
            P(None, "tp"),
            P("tp"),
            P(None, "tp"),
            P(None, "tp"),
            P(None, "tp"),
            P("tp", None),
            P("tp", None),
            P("tp"),
            P(),
            P("tp", None),
            P("tp", None),
        ),
        out_specs=(P(("sp", "tp"), None), P(None, "tp", "sp")),
        check_vma=False,
    )
```

```python
import functools

import jax
import jax.numpy as jnp
from jax import lax
from jax.experimental import pallas as pl
from jax.experimental.pallas import tpu as pltpu
from jax.sharding import PartitionSpec as P

KW = 31
HALO = 32
LOG2_E = 1.4426950408889634
LN_2 = 0.6931471805599453
F32 = jnp.float32
BF16 = jnp.bfloat16
MESH = pl.DeviceIdType.MESH


def dot(a, b):
    return jnp.dot(a, b, preferred_element_type=F32)


def kernel(
    sp_n,
    tp_n,
    tokens_hbm,
    norm_gain_hbm,
    w_glu_a,
    w_glu_b,
    taps_hbm,
    ln_gain_hbm,
    w_query,
    w_key,
    w_value,
    q_gain_hbm,
    k_gain_hbm,
    lam_hbm,
    sub_gain_hbm,
    w_out_conv,
    w_out_attn,
    mixed,
    logs,
    tokens,
    norm_gain,
    taps,
    ln_gain,
    q_gain,
    k_gain,
    lam,
    sub_gain,
    wa,
    wb,
    wq,
    wkv,
    woc,
    woa,
    nrm,
    kv,
    qtz,
    gat,
    halo_s,
    halo_r,
    conv,
    st,
    stat,
    c_out,
    m_ref,
    l_ref,
    acc,
    a_out,
    part,
    mate_s,
    mate_r,
    y_s,
    y_r,
    w_sem,
    ag_send,
    ag_recv,
    z_send,
    x_send,
    kv_recv,
    halo_sem,
    stat_send,
    stat_recv,
    mate_send,
    mate_recv,
    y_send,
    y_recv,
):
    sp = lax.axis_index("sp")
    tp = lax.axis_index("tp")
    rows = tokens.shape[0]
    width = tokens.shape[1]
    tok = rows * tp_n
    half_rows = tok // 2
    heads = q_gain.shape[0]
    vdim = sub_gain.shape[1]
    hd = q_gain.shape[1] // 2
    chans = taps.shape[1]
    core = tp % 2
    y = tp // 2
    yo = 1 - y
    mate = tp + 1 - 2 * core
    cross = (tp + 2) % 4
    lane = sp % 2
    pos = sp // 2
    npos = sp_n // 2
    xmate = sp + 1 - 2 * lane

    bar = pltpu.get_barrier_semaphore()

    def greet_sp(i, c):
        pl.semaphore_signal(bar, inc=1, device_id=((sp + i) % sp_n, tp), device_id_type=MESH)
        return c

    lax.fori_loop(1, sp_n, greet_sp, 0)
    for i in range(1, tp_n):
        pl.semaphore_signal(bar, inc=1, device_id=(sp, (tp + i) % tp_n), device_id_type=MESH)

    kw = w_key.shape[1]
    loads = [
        pltpu.make_async_copy(src, dst, w_sem.at[i])
        for i, (src, dst) in enumerate(
            [
                (tokens_hbm, tokens),
                (norm_gain_hbm, norm_gain),
                (w_key, wkv.at[:, :kw]),
                (w_value, wkv.at[:, kw:]),
                (k_gain_hbm, k_gain),
                (w_glu_a, wa),
                (w_glu_b, wb),
                (q_gain_hbm, q_gain),
                (w_query, wq),
                (taps_hbm, taps),
                (ln_gain_hbm, ln_gain),
                (w_out_conv, woc),
                (sub_gain_hbm, sub_gain),
                (lam_hbm, lam),
                (w_out_attn, woa),
            ]
        )
    ]
    for copy in loads:
        copy.start()

    def loaded(lo, hi):
        for copy in loads[lo:hi]:
            copy.wait()

    qtz[...] = jnp.zeros_like(qtz)
    loaded(0, 2)
    x = tokens[...].astype(F32)
    scale = lax.rsqrt(jnp.mean(x * x, axis=-1, keepdims=True) + 1e-06)
    nrm[tp] = (x * scale * norm_gain[...]).astype(BF16)
    pl.semaphore_wait(bar, sp_n - 1 + tp_n - 1)

    ag_chunks = 4

    def ag_copy(slot, k, i, target):
        piece = pl.ds((ag_chunks - 1 - i) * (rows // ag_chunks), rows // ag_chunks)
        return pltpu.make_async_remote_copy(
            src_ref=nrm.at[slot, piece],
            dst_ref=nrm.at[slot, piece],
            send_sem=ag_send.at[k, i],
            recv_sem=ag_recv.at[k, i],
            device_id=(sp, target),
            device_id_type=MESH,
        )

    ag_cross = [ag_copy(tp, 0, i, cross) for i in range(ag_chunks)]
    ag_mate = [
        pltpu.make_async_remote_copy(
            src_ref=nrm.at[tp],
            dst_ref=nrm.at[tp],
            send_sem=ag_send.at[1, 0],
            recv_sem=ag_recv.at[1, 0],
            device_id=(sp, mate),
            device_id_type=MESH,
        )
    ]
    ag_fwd = [ag_copy(cross, 2, i, mate) for i in range(ag_chunks)]
    for copy in ag_cross + ag_mate:
        copy.start()

    def half_in(h):
        return nrm[pl.ds(2 * h, 2)].reshape(half_rows, width)

    def norm_kv(xin):
        res = dot(xin, wkv[...])
        k = res[:, :kw]
        first = lax.broadcasted_iota(jnp.int32, k.shape, 1) < hd
        sq = k * k
        s0 = jnp.sum(jnp.where(first, sq, 0.0), axis=1, keepdims=True)
        s1 = jnp.sum(jnp.where(first, 0.0, sq), axis=1, keepdims=True)
        r = jnp.where(first, lax.rsqrt(s0 / hd + 1e-06), lax.rsqrt(s1 / hd + 1e-06))
        return (k * r * k_gain[...]).astype(BF16), res[:, kw:].astype(BF16)

    half_slot = rows // 2

    def first_row(i):
        return (1 - i) * half_slot

    def unit_in(i):
        at = slice(first_row(i), first_row(i) + half_slot)
        return jnp.concatenate([nrm[2 * yo, at, :], nrm[2 * yo + 1, at, :]], axis=0)

    def proj_kv_near():
        k, v = norm_kv(half_in(y))
        for i in range(2):
            for j in range(2):
                src = slice(j * rows + first_row(i), j * rows + first_row(i) + half_slot)
                dst = slice(j * half_slot, (j + 1) * half_slot)
                kv[sp, 2 * y + i, dst, :] = k[src]
                kv[sp, 2 * y + i, rows + j * half_slot : rows + (j + 1) * half_slot, :] = v[src]

    def proj_kv_far(i):
        k, v = norm_kv(unit_in(i))
        kv[sp, 2 * yo + i, :rows, :] = k
        kv[sp, 2 * yo + i, rows:, :] = v

    def kv_part(s, m):
        if m == 0:
            return kv.at[s, pl.ds(2 * y, 2)]
        return kv.at[s, pl.ds(2 * yo + m - 1, 1)]

    def z_copy(p, m, d):
        s = p * 2 + lane
        return pltpu.make_async_remote_copy(
            src_ref=kv_part(s, m),
            dst_ref=kv_part(s, m),
            send_sem=z_send.at[p, m, d - 1],
            recv_sem=kv_recv.at[s, m],
            device_id=((pos + d) * 2 + lane, tp),
            device_id_type=MESH,
        )

    last = pos == npos - 1

    def x_copy(p, m):
        s = p * 2 + lane
        return pltpu.make_async_remote_copy(
            src_ref=kv_part(s, m),
            dst_ref=kv_part(s, m),
            send_sem=x_send.at[p, m],
            recv_sem=kv_recv.at[s, m],
            device_id=(xmate, tp),
            device_id_type=MESH,
        )

    def arrived(s, m):
        pltpu.make_async_remote_copy(
            src_ref=kv_part(s, m),
            dst_ref=kv_part(s, m),
            send_sem=x_send.at[0, m],
            recv_sem=kv_recv.at[s, m],
            device_id=(xmate, tp),
            device_id_type=MESH,
        ).wait_recv()

    late = 2

    def direct_kv(then):
        def one(i, c):
            then(z_copy(pos, late, npos - 1 - pos - i))
            return c

        lax.fori_loop(0, npos - 1 - pos, one, 0)

    def tree_kv(p, m, then):
        @pl.when((p == pos) & (pos + 2 < npos))
        def _():
            then(z_copy(p, m, 2))

        @pl.when((p != pos - 1) & (pos + 1 < npos))
        def _():
            then(z_copy(p, m, 1))

    def send_kv(m):
        if m == late:
            direct_kv(lambda copy: copy.start())
        else:
            tree_kv(pos, m, lambda copy: copy.start())

        @pl.when(lane == 0)
        def _():
            x_copy(pos, m).start()

    def relay_kv(m, lo, hi=None, along=True, across=True):
        def one(i, c):
            p = pos - 1 - i
            if along:
                arrived(p * 2 + lane, m)
                if m != late:
                    tree_kv(p, m, lambda copy: copy.start())
            if across:
                x_copy(p, m).start()
            return c

        lax.fori_loop(lo, pos if hi is None else jnp.minimum(pos, hi), one, 0)

    def relay_last(m, lo, hi):
        relay_kv(m, lo, jnp.where(last, hi, 0))

    def relay_rest(m, lo, hi, along=True, across=True):
        relay_kv(m, lo, jnp.where(last, 0, hi), along, across)

    def gate(xin, n):
        wide = 256
        cols = slice(n * wide, (n + 1) * wide)
        a = dot(xin, wa[:, cols])
        b = dot(xin, wb[:, cols])
        return (a * jax.nn.sigmoid(b)).astype(BF16)

    def proj_glu_near():
        xin = half_in(y)
        at = pl.ds(pl.multiple_of(HALO + y * half_rows, HALO), half_rows)
        for n in range(chans // 256):
            g = gate(xin, n)
            for j in range(2):
                gat[2 * n + j, at, :] = g[:, j * 128 : (j + 1) * 128].astype(F32)

            @pl.when(y == 1)
            def _():
                halo_s[:, n * 256 : (n + 1) * 256] = g[half_rows - HALO :, :]

    def proj_glu_far(i):
        xin = unit_in(i)
        for n in range(chans // 256):
            g = gate(xin, n)
            for t in range(2):
                at = pl.ds(pl.multiple_of(HALO + yo * half_rows + t * rows + first_row(i), HALO), half_slot)
                part_g = g[t * half_slot : (t + 1) * half_slot]
                for j in range(2):
                    gat[2 * n + j, at, :] = part_g[:, j * 128 : (j + 1) * 128].astype(F32)
            if i == 0:

                @pl.when(yo == 1)
                def _():
                    halo_s[:, n * 256 : (n + 1) * 256] = g[rows - HALO : rows, :]

    def proj_q(h):
        xin = half_in(h)

        def one(n, c):
            q = dot(xin, wq[:, pl.ds(pl.multiple_of(n * 4 * hd, 4 * hd), 4 * hd)])
            qt = q.T.reshape(4, hd, half_rows)
            r = lax.rsqrt(jnp.mean(qt * qt, axis=1, keepdims=True) + 1e-06)
            qn = qt * r
            for j in range(2):
                gain = jnp.broadcast_to(q_gain[pl.ds(n * 2 + j, 1), :], (2 * hd, 2 * hd)).T
                for m in range(2):
                    gm = gain[m * hd : (m + 1) * hd, :half_rows]
                    val = (qn[j * 2 + m] * gm).astype(BF16).astype(F32) * (hd ** (-0.5) * LOG2_E)
                    high = val.astype(BF16)
                    low = (val - high.astype(F32)).astype(BF16)
                    first = (n * 2 + j) * tok + m * half_rows
                    lanes = pl.ds(pl.multiple_of(first, half_rows), half_rows)
                    qtz[h, m * hd : (m + 1) * hd, lanes] = high
                    qtz[h, (m + 2) * hd : (m + 3) * hd, lanes] = low
            return c

        for n in range(heads // 2):
            one(n, 0)

    def halo_copy():
        return pltpu.make_async_remote_copy(
            src_ref=halo_s,
            dst_ref=halo_r,
            send_sem=halo_sem.at[0],
            recv_sem=halo_sem.at[1],
            device_id=((sp + 1) % sp_n, tp),
            device_id_type=MESH,
        )

    def send_halo(h):
        @pl.when((sp < sp_n - 1) & (h == 1))
        def _():
            halo_copy().start()

    loaded(2, 5)
    ag_mate[0].wait_recv()
    proj_kv_near()
    send_kv(0)
    loaded(5, 7)
    proj_glu_near()
    send_halo(y)
    loaded(7, 9)
    proj_q(y)

    def far_row(n):
        ag_cross[n].wait_recv()
        ag_fwd[n].start()

    far_row(0)
    far_row(1)
    ag_fwd[0].wait_recv()
    ag_fwd[1].wait_recv()
    proj_kv_far(0)
    send_kv(1)
    relay_rest(0, 1, npos, across=False)
    far_row(2)

    @pl.when(core == 1)
    def _():
        far_row(3)

    proj_glu_far(0)
    send_halo(yo)
    @pl.when(core == 0)
    def _():
        far_row(3)

    relay_rest(0, 0, 1)
    relay_rest(0, 1, npos, along=False)
    relay_last(0, 0, 2)
    ag_fwd[2].wait_recv()
    ag_fwd[3].wait_recv()
    proj_kv_far(1)
    send_kv(2)
    proj_glu_far(1)
    def attend(blocks, q, diag, units=(0, 1, 2, 3)):
        keys = jnp.concatenate([kv[s, u, :rows, :] for s in blocks for u in units], axis=0)
        vals = jnp.concatenate([kv[s, u, rows:, :] for s in blocks for u in units], axis=0).T
        if diag:
            e = lax.broadcasted_iota(jnp.int32, (tok, 1), 0)
            kpos = e // half_rows * half_rows + e // half_slot % 2 * rows
            kpos = kpos + (1 - e // rows % 2) * half_slot + e % half_slot
            qpos = lax.broadcasted_iota(jnp.int32, (1, tok), 1)
            qpos = jnp.where(qpos >= half_rows, qpos - half_rows, qpos) + q * half_rows
            seen = kpos <= qpos
        every = dot(jnp.concatenate([keys, keys], axis=1), qtz[q])
        for h in range(heads):
            sc = every[:, h * tok : (h + 1) * tok]
            if diag:
                sc = jnp.where(seen, sc, -1e30)
                top = jnp.max(sc, axis=0, keepdims=True)
                wgt = jnp.exp2(sc - top)
                l_ref[h][q] = jnp.sum(wgt, axis=0, keepdims=True)
                acc[h][q] = dot(vals, wgt.astype(BF16))
            else:
                old = m_ref[h][q]
                top = jnp.maximum(old, jnp.max(sc, axis=0, keepdims=True))
                wgt = jnp.exp2(sc - top)
                alpha = jnp.exp2(old - top)
                l_ref[h][q] = l_ref[h][q] * alpha + jnp.sum(wgt, axis=0, keepdims=True)
                acc[h][q] = acc[h][q] * alpha + dot(vals, wgt.astype(BF16))
            m_ref[h][q] = top

    step_rows = 64
    loaded(9, 10)

    def conv_half(h):
        @pl.when((h == 0) & (sp > 0))
        def _():
            halo_copy().wait_recv()
            for j in range(chans // 128):
                gat[j, :HALO, :] = halo_r[:, j * 128 : (j + 1) * 128].astype(F32)

        @pl.when((h == 0) & (sp == 0))
        def _():
            gat[:, :HALO, :] = jnp.zeros((chans // 128, HALO, 128), F32)

        st[...] = jnp.zeros_like(st)

        def conv_cols(cc, c):
            cols = pl.ds(pl.multiple_of(cc * 128, 128), 128)
            rows_in = gat.at[cc, pl.ds(pl.multiple_of(h * half_rows, half_rows), HALO + half_rows), :]
            rows_out = conv.at[cc, pl.ds(pl.multiple_of(h * half_rows, half_rows), half_rows), :]
            for r0 in range(0, half_rows, step_rows):
                total = jnp.zeros((step_rows, 128), F32)
                for j in range(KW):
                    first = r0 + HALO - KW + 1 + j
                    total = total + taps[j : j + 1, cols] * rows_in[first : first + step_rows, :]
                rows_out[r0 : r0 + step_rows, :] = total
                st[0, r0 : r0 + step_rows, :] += total
                st[1, r0 : r0 + step_rows, :] += total * total
            return c

        lax.fori_loop(0, chans // 128, conv_cols, 0)
        stat[h, tp] = jnp.concatenate(
            [jnp.sum(st[i].T, axis=0, keepdims=True) for i in range(2)], axis=0
        )
        for i in range(1, tp_n):
            stat_copy(h, i).start()

    def stat_copy(h, i):
        return pltpu.make_async_remote_copy(
            src_ref=stat.at[h, tp],
            dst_ref=stat.at[h, tp],
            send_sem=stat_send.at[h, i],
            recv_sem=stat_recv.at[h, i],
            device_id=(sp, (tp + i) % tp_n),
            device_id_type=MESH,
        )

    wide = y_s.shape[2]
    chunks = width // wide

    def half_of(h):
        return pl.ds(pl.multiple_of(h * half_rows, half_rows), half_rows)

    def close_conv(h):
        for i in range(1, tp_n):
            stat_copy(h, i).wait_recv()
        sums = stat[h, 0]
        for i in range(1, tp_n):
            sums = sums + stat[h, i]
        sums = sums / (chans * tp_n)
        mu = sums[0:1]
        inv = lax.rsqrt(sums[1:2] - mu * mu + 1e-05)
        mu_t = jnp.broadcast_to(mu, (128, half_rows)).T
        inv_t = jnp.broadcast_to(inv, (128, half_rows)).T
        for cc in range(chans // 128):
            cols = slice(cc * 128, (cc + 1) * 128)
            val = (conv[cc, half_of(h), :] - mu_t) * inv_t * ln_gain[:, cols]
            c_out[half_of(h), cols] = (val * jax.nn.sigmoid(val)).astype(BF16)

    def out_conv(h):
        for n in range(chunks):
            cols = slice(n * wide, (n + 1) * wide)
            part[half_of(h), cols] = dot(c_out[half_of(h), :], woc[:, cols])

    relay_rest(1, 0, 1)
    conv_half(yo)
    relay_rest(1, 1, npos)
    relay_last(1, 0, 2)
    tail = last & (lane == 0) & (pos > 0)

    @pl.when(jnp.logical_not(tail))
    def _():
        conv_half(y)

    relay_last(0, 2, npos)
    proj_q(yo)
    attend([sp], yo, True)
    relay_rest(2, 0, 1)
    relay_last(2, 0, 1)

    @pl.when(lane == 1)
    def _():
        for m in range(3):
            arrived(sp - 1, m)
        attend([sp - 1], yo, False)
        relay_last(1, 2, npos)
        relay_last(2, 1, 2)

    def near_attn():
        attend([sp], y, True)

        @pl.when(lane == 1)
        def _():
            attend([sp - 1], y, False)

    def near_conv():
        close_conv(y)
        out_conv(y)

    @pl.when(tail)
    def _():
        conv_half(y)

    relay_rest(2, 1, npos)
    pl.when(pos > 0)(near_attn)

    @pl.when(lane == 0)
    def _():
        relay_last(1, 2, npos)
        relay_last(2, 1, 2)

    relay_last(2, 2, npos)

    def pairs_far():
        def one(i, c):
            p = pos - 1 - i
            for m in range(3):
                arrived(p * 2 + 1 - lane, m)
            attend([p * 2, p * 2 + 1], yo, False)
            return c

        loaded(10, 11)
        close_conv(yo)
        loaded(11, 12)
        out_conv(yo)
        pl.when((pos > 0) & jnp.logical_not(tail))(near_conv)
        lax.fori_loop(0, pos, one, 0)

    def pairs_near():
        def one(i, c):
            p = pos - 1 - i
            attend([p * 2, p * 2 + 1], y, False)
            return c

        lax.fori_loop(0, pos, one, 0)

    loaded(12, 15)
    sub_t = jnp.broadcast_to(sub_gain[...], (half_rows, vdim)).T

    def close_heads(q):
        at = pl.ds(pl.multiple_of(q * half_rows, half_rows), half_rows)
        for h in range(heads):
            total = l_ref[h][q]
            log_row = m_ref[h][q] * LN_2 + jnp.log(total)
            maps = acc[h][q] / total
            for m in range(2):
                logs[m, h : h + 1, at] = log_row[:, m * half_rows : (m + 1) * half_rows]
            diff = maps[:, :half_rows] - lam[h] * maps[:, half_rows:]
            out = diff * lax.rsqrt(jnp.mean(diff * diff, axis=0, keepdims=True) + 1e-06) * sub_t
            a_out[at, h * vdim : (h + 1) * vdim] = out.T.astype(BF16)

    def mate_copy(k, n):
        return pltpu.make_async_remote_copy(
            src_ref=mate_s.at[k, n],
            dst_ref=mate_r.at[k, n],
            send_sem=mate_send.at[k, n],
            recv_sem=mate_recv.at[k, n],
            device_id=(sp, mate),
            device_id_type=MESH,
        )

    def y_copy(n):
        return pltpu.make_async_remote_copy(
            src_ref=y_s.at[n],
            dst_ref=y_r.at[n],
            send_sem=y_send.at[n],
            recv_sem=y_recv.at[n],
            device_id=(sp, cross),
            device_id_type=MESH,
        )

    def owner_rows(h, c):
        return pl.ds(pl.multiple_of((h * 2 + c) * rows, rows), rows)

    def out_attn(k, h):
        for piece in (range(0, 1), range(1, chunks)):
            for n in piece:
                cols = slice(n * wide, (n + 1) * wide)
                part[half_of(h), cols] += dot(a_out[half_of(h), :], woa[:, cols])
            for n in piece:
                cols = slice(n * wide, (n + 1) * wide)
                mate_s[k, n] = part[owner_rows(h, 1 - core), cols].astype(BF16)
                mate_copy(k, n).start()

    pairs_far()
    close_heads(yo)
    out_attn(0, yo)

    def forward(n, c):
        cols = pl.ds(pl.multiple_of(n * wide, wide), wide)
        mate_copy(0, n).wait_recv()
        y_s[n] = (part[owner_rows(yo, core), cols] + mate_r[0, n].astype(F32)).astype(BF16)
        y_copy(n).start()
        return c

    lax.fori_loop(0, chunks, forward, 0)

    @pl.when(pos == 0)
    def _():
        near_attn()

    pl.when((pos == 0) | tail)(near_conv)

    pairs_near()
    close_heads(y)
    out_attn(1, y)

    def finish(n, c):
        cols = pl.ds(pl.multiple_of(n * wide, wide), wide)
        mate_copy(1, n).wait_recv()
        y_copy(n).wait_recv()
        total = part[owner_rows(y, core), cols] + mate_r[1, n].astype(F32) + y_r[n].astype(F32)
        mixed[:, cols] = total.astype(BF16)
        return c

    for copy in ag_cross + ag_mate + ag_fwd:
        copy.wait_send()
    for h in range(2):
        for i in range(1, tp_n):
            stat_copy(h, i).wait_send()

    @pl.when(sp < sp_n - 1)
    def _():
        halo_copy().wait_send()

    for m in range(3):

        @pl.when(lane == 0)
        def _():
            x_copy(pos, m).wait_send()

        if m == late:
            direct_kv(lambda copy: copy.wait_send())
        else:
            tree_kv(pos, m, lambda copy: copy.wait_send())

        def relay_done(p, c):
            x_copy(p, m).wait_send()
            if m != late:
                tree_kv(p, m, lambda copy: copy.wait_send())
            return c

        lax.fori_loop(0, pos, relay_done, 0)
    lax.fori_loop(0, chunks, finish, 0)

    def rs_done(n, c):
        mate_copy(0, n).wait_send()
        mate_copy(1, n).wait_send()
        y_copy(n).wait_send()
        return c

    lax.fori_loop(0, chunks, rs_done, 0)


def put_out(mixed, logs, mixed_hbm, logs_hbm, sem):
    copies = [
        pltpu.make_async_copy(mixed, mixed_hbm, sem.at[0]),
        pltpu.make_async_copy(logs, logs_hbm, sem.at[1]),
    ]
    for copy in copies:
        copy.start()
    for copy in copies:
        copy.wait()


def on_device(sp_n, tp_n, *args):
    (
        tokens,
        norm_gain,
        w_glu_a,
        w_glu_b,
        conv_taps,
        ln_gain,
        w_query,
        w_key,
        w_value,
        query_gain,
        key_gain,
        lam_head,
        sub_gain,
        w_out_conv,
        w_out_attn,
    ) = args
    rows, width = tokens.shape
    tok = rows * tp_n
    half = tok // 2
    chans = conv_taps.shape[1]
    heads = lam_head.shape[0]
    qcols = w_query.shape[1]
    kcols = w_key.shape[1]
    vcols = w_value.shape[1]
    vdim = sub_gain.shape[0]
    acols = w_out_attn.shape[0]
    chunks = 4
    wide = width // chunks
    vmem = pl.BlockSpec(memory_space=pltpu.VMEM)
    dma = pltpu.SemaphoreType.DMA
    hbm = pl.BlockSpec(memory_space=pltpu.HBM)
    mixed, logs = pl.pallas_call(
        functools.partial(kernel, sp_n, tp_n),
        out_shape=(
            pltpu.VMEM((rows, width), BF16),
            pltpu.VMEM((2, heads, tok), F32),
        ),
        in_specs=[hbm] * 15,
        out_specs=(vmem, vmem),
        scratch_shapes=[
            pltpu.VMEM((rows, width), BF16),
            pltpu.VMEM((1, width), F32),
            pltpu.VMEM(conv_taps.shape, F32),
            pltpu.VMEM((1, chans), F32),
            pltpu.VMEM(query_gain.shape, F32),
            pltpu.VMEM(key_gain.shape, F32),
            pltpu.SMEM((heads,), F32),
            pltpu.VMEM((1, vdim), F32),
            pltpu.VMEM((width, chans), BF16),
            pltpu.VMEM((width, chans), BF16),
            pltpu.VMEM((width, qcols), BF16),
            pltpu.VMEM((width, kcols + vcols), BF16),
            pltpu.VMEM((chans, width), BF16),
            pltpu.VMEM((acols, width), BF16),
            pltpu.VMEM((tp_n, rows, width), BF16),
            pltpu.VMEM((sp_n, 4, 2 * rows, kcols), BF16),
            pltpu.VMEM((2, 2 * kcols, heads * tok), BF16),
            pltpu.VMEM((chans // 128, HALO + tok, 128), F32),
            pltpu.VMEM((HALO, chans), BF16),
            pltpu.VMEM((HALO, chans), BF16),
            pltpu.VMEM((chans // 128, tok, 128), F32),
            pltpu.VMEM((2, half, 128), F32),
            pltpu.VMEM((2, tp_n, 2, half), F32),
            pltpu.VMEM((tok, chans), BF16),
            [pltpu.VMEM((2, 1, tok), F32) for _ in range(heads)],
            [pltpu.VMEM((2, 1, tok), F32) for _ in range(heads)],
            [pltpu.VMEM((2, vdim, tok), F32) for _ in range(heads)],
            pltpu.VMEM((tok, acols), BF16),
            pltpu.VMEM((tok, width), F32),
            pltpu.VMEM((2, chunks, rows, wide), BF16),
            pltpu.VMEM((2, chunks, rows, wide), BF16),
            pltpu.VMEM((chunks, rows, wide), BF16),
            pltpu.VMEM((chunks, rows, wide), BF16),
            dma((15,)),
            dma((3, 4)),
            dma((3, 4)),
            dma((sp_n // 2, 3, max(2, sp_n // 2 - 1))),
            dma((sp_n // 2, 3)),
            dma((sp_n, 3)),
            dma((2,)),
            dma((2, tp_n)),
            dma((2, tp_n)),
            dma((2, chunks)),
            dma((2, chunks)),
            dma((chunks,)),
            dma((chunks,)),
        ],
        compiler_params=pltpu.CompilerParams(
            collective_id=0, has_side_effects=True, vmem_limit_bytes=56 * 2**20
        ),
    )(
        tokens,
        norm_gain.reshape(1, -1),
        w_glu_a,
        w_glu_b,
        conv_taps,
        ln_gain.reshape(1, -1),
        w_query,
        w_key,
        w_value,
        query_gain,
        key_gain,
        lam_head,
        sub_gain.reshape(1, -1),
        w_out_conv,
        w_out_attn,
    )
    return pl.pallas_call(
        put_out,
        out_shape=(
            jax.ShapeDtypeStruct((rows, width), BF16),
            jax.ShapeDtypeStruct((2, heads, tok), F32),
        ),
        in_specs=[vmem, vmem],
        out_specs=(hbm, hbm),
        scratch_shapes=[dma((2,))],
    )(
        pltpu.with_memory_space_constraint(mixed, pltpu.VMEM),
        pltpu.with_memory_space_constraint(logs, pltpu.VMEM),
    )


def solution(mesh):
    return jax.shard_map(
        functools.partial(on_device, mesh.shape["sp"], mesh.shape["tp"]),
        mesh=mesh,
        in_specs=(
            P(("sp", "tp"), None),
            P(),
            P(None, "tp"),
            P(None, "tp"),
            P(None, "tp"),
            P("tp"),
            P(None, "tp"),
            P(None, "tp"),
            P(None, "tp"),
            P("tp", None),
            P("tp", None),
            P("tp"),
            P(),
            P("tp", None),
            P("tp", None),
        ),
        out_specs=(P(("sp", "tp"), None), P(None, "tp", "sp")),
        check_vma=False,
    )
```

```python
import functools

import jax
import jax.numpy as jnp
from jax import lax
from jax.experimental import pallas as pl
from jax.experimental.pallas import tpu as pltpu
from jax.sharding import PartitionSpec as P

KW = 31
HALO = 32
LOG2_E = 1.4426950408889634
LN_2 = 0.6931471805599453
F32 = jnp.float32
BF16 = jnp.bfloat16
MESH = pl.DeviceIdType.MESH


def dot(a, b):
    return jnp.dot(a, b, preferred_element_type=F32)


def kernel(
    sp_n,
    tp_n,
    tokens_hbm,
    norm_gain_hbm,
    w_glu_a,
    w_glu_b,
    taps_hbm,
    ln_gain_hbm,
    w_query,
    w_key,
    w_value,
    q_gain_hbm,
    k_gain_hbm,
    lam_hbm,
    sub_gain_hbm,
    w_out_conv,
    w_out_attn,
    mixed,
    logs,
    tokens,
    norm_gain,
    taps,
    ln_gain,
    q_gain,
    k_gain,
    lam,
    sub_gain,
    wa,
    wb,
    wq,
    wkv,
    woc,
    woa,
    nrm,
    kv,
    qtz,
    gat,
    halo_s,
    halo_r,
    conv,
    st,
    stat,
    c_out,
    m_ref,
    l_ref,
    acc,
    a_out,
    part,
    mate_s,
    mate_r,
    y_s,
    y_r,
    w_sem,
    ag_send,
    ag_recv,
    z_send,
    x_send,
    kv_recv,
    halo_sem,
    stat_send,
    stat_recv,
    mate_send,
    mate_recv,
    y_send,
    y_recv,
):
    sp = lax.axis_index("sp")
    tp = lax.axis_index("tp")
    rows = tokens.shape[0]
    width = tokens.shape[1]
    tok = rows * tp_n
    half_rows = tok // 2
    heads = q_gain.shape[0]
    vdim = sub_gain.shape[1]
    hd = q_gain.shape[1] // 2
    chans = taps.shape[1]
    core = tp % 2
    y = tp // 2
    yo = 1 - y
    mate = tp + 1 - 2 * core
    cross = (tp + 2) % 4
    lane = sp % 2
    pos = sp // 2
    npos = sp_n // 2
    xmate = sp + 1 - 2 * lane

    bar = pltpu.get_barrier_semaphore()

    def greet_sp(i, c):
        pl.semaphore_signal(bar, inc=1, device_id=((sp + i) % sp_n, tp), device_id_type=MESH)
        return c

    lax.fori_loop(1, sp_n, greet_sp, 0)
    for i in range(1, tp_n):
        pl.semaphore_signal(bar, inc=1, device_id=(sp, (tp + i) % tp_n), device_id_type=MESH)

    kw = w_key.shape[1]
    loads = [
        pltpu.make_async_copy(src, dst, w_sem.at[i])
        for i, (src, dst) in enumerate(
            [
                (tokens_hbm, tokens),
                (norm_gain_hbm, norm_gain),
                (w_key, wkv.at[:, :kw]),
                (w_value, wkv.at[:, kw:]),
                (k_gain_hbm, k_gain),
                (w_glu_a, wa),
                (w_glu_b, wb),
                (q_gain_hbm, q_gain),
                (w_query, wq),
                (taps_hbm, taps),
                (ln_gain_hbm, ln_gain),
                (w_out_conv, woc),
                (sub_gain_hbm, sub_gain),
                (lam_hbm, lam),
                (w_out_attn, woa),
            ]
        )
    ]
    for copy in loads:
        copy.start()

    def loaded(lo, hi):
        for copy in loads[lo:hi]:
            copy.wait()

    qtz[...] = jnp.zeros_like(qtz)
    loaded(0, 2)
    x = tokens[...].astype(F32)
    scale = lax.rsqrt(jnp.mean(x * x, axis=-1, keepdims=True) + 1e-06)
    nrm[tp] = (x * scale * norm_gain[...]).astype(BF16)
    pl.semaphore_wait(bar, sp_n - 1 + tp_n - 1)

    ag_chunks = 4

    def ag_copy(slot, k, i, target):
        piece = pl.ds((ag_chunks - 1 - i) * (rows // ag_chunks), rows // ag_chunks)
        return pltpu.make_async_remote_copy(
            src_ref=nrm.at[slot, piece],
            dst_ref=nrm.at[slot, piece],
            send_sem=ag_send.at[k, i],
            recv_sem=ag_recv.at[k, i],
            device_id=(sp, target),
            device_id_type=MESH,
        )

    ag_cross = [ag_copy(tp, 0, i, cross) for i in range(ag_chunks)]
    ag_mate = [
        pltpu.make_async_remote_copy(
            src_ref=nrm.at[tp],
            dst_ref=nrm.at[tp],
            send_sem=ag_send.at[1, 0],
            recv_sem=ag_recv.at[1, 0],
            device_id=(sp, mate),
            device_id_type=MESH,
        )
    ]
    ag_fwd = [ag_copy(cross, 2, i, mate) for i in range(ag_chunks)]
    for copy in ag_cross[:2] + ag_mate:
        copy.start()

    def half_in(h):
        return nrm[pl.ds(2 * h, 2)].reshape(half_rows, width)

    def norm_kv(xin):
        res = dot(xin, wkv[...])
        k = res[:, :kw]
        first = lax.broadcasted_iota(jnp.int32, k.shape, 1) < hd
        sq = k * k
        s0 = jnp.sum(jnp.where(first, sq, 0.0), axis=1, keepdims=True)
        s1 = jnp.sum(jnp.where(first, 0.0, sq), axis=1, keepdims=True)
        r = jnp.where(first, lax.rsqrt(s0 / hd + 1e-06), lax.rsqrt(s1 / hd + 1e-06))
        return (k * r * k_gain[...]).astype(BF16), res[:, kw:].astype(BF16)

    half_slot = rows // 2

    def first_row(i):
        return (1 - i) * half_slot

    def unit_in(i):
        at = slice(first_row(i), first_row(i) + half_slot)
        return jnp.concatenate([nrm[2 * yo, at, :], nrm[2 * yo + 1, at, :]], axis=0)

    def proj_kv_near():
        k, v = norm_kv(half_in(y))
        for i in range(2):
            for j in range(2):
                src = slice(j * rows + first_row(i), j * rows + first_row(i) + half_slot)
                dst = slice(j * half_slot, (j + 1) * half_slot)
                kv[sp, 2 * y + i, dst, :] = k[src]
                kv[sp, 2 * y + i, rows + j * half_slot : rows + (j + 1) * half_slot, :] = v[src]

    def proj_kv_far(i):
        k, v = norm_kv(unit_in(i))
        kv[sp, 2 * yo + i, :rows, :] = k
        kv[sp, 2 * yo + i, rows:, :] = v

    def kv_part(s, m):
        if m == 0:
            return kv.at[s, pl.ds(2 * y, 2)]
        return kv.at[s, pl.ds(2 * yo + m - 1, 1)]

    def z_copy(p, m, d):
        s = p * 2 + lane
        return pltpu.make_async_remote_copy(
            src_ref=kv_part(s, m),
            dst_ref=kv_part(s, m),
            send_sem=z_send.at[p, m, d - 1],
            recv_sem=kv_recv.at[s, m],
            device_id=((pos + d) * 2 + lane, tp),
            device_id_type=MESH,
        )

    last = pos == npos - 1

    def x_copy(p, m):
        s = p * 2 + lane
        return pltpu.make_async_remote_copy(
            src_ref=kv_part(s, m),
            dst_ref=kv_part(s, m),
            send_sem=x_send.at[p, m],
            recv_sem=kv_recv.at[s, m],
            device_id=(xmate, tp),
            device_id_type=MESH,
        )

    def arrived(s, m):
        pltpu.make_async_remote_copy(
            src_ref=kv_part(s, m),
            dst_ref=kv_part(s, m),
            send_sem=x_send.at[0, m],
            recv_sem=kv_recv.at[s, m],
            device_id=(xmate, tp),
            device_id_type=MESH,
        ).wait_recv()

    late = 2

    def direct_kv(then):
        def one(i, c):
            then(z_copy(pos, late, npos - 1 - pos - i))
            return c

        lax.fori_loop(0, npos - 1 - pos, one, 0)

    def tree_kv(p, m, then):
        @pl.when((p == pos) & (pos + 2 < npos))
        def _():
            then(z_copy(p, m, 2))

        @pl.when((p != pos - 1) & (pos + 1 < npos))
        def _():
            then(z_copy(p, m, 1))

    def send_kv(m):
        if m == late:
            direct_kv(lambda copy: copy.start())
        else:
            tree_kv(pos, m, lambda copy: copy.start())

        @pl.when(lane == 0)
        def _():
            x_copy(pos, m).start()

    def relay_kv(m, lo, hi=None, along=True, across=True):
        def one(i, c):
            p = pos - 1 - i
            if along:
                arrived(p * 2 + lane, m)
                if m != late:
                    tree_kv(p, m, lambda copy: copy.start())
            if across:
                x_copy(p, m).start()
            return c

        lax.fori_loop(lo, pos if hi is None else jnp.minimum(pos, hi), one, 0)

    def relay_last(m, lo, hi):
        relay_kv(m, lo, jnp.where(last, hi, 0))

    def relay_rest(m, lo, hi, along=True, across=True):
        relay_kv(m, lo, jnp.where(last, 0, hi), along, across)

    def gate(xin, n):
        wide = 256
        cols = slice(n * wide, (n + 1) * wide)
        a = dot(xin, wa[:, cols])
        b = dot(xin, wb[:, cols])
        return (a * jax.nn.sigmoid(b)).astype(BF16)

    def proj_glu_near():
        xin = half_in(y)
        at = pl.ds(pl.multiple_of(HALO + y * half_rows, HALO), half_rows)
        for n in range(chans // 256):
            g = gate(xin, n)
            for j in range(2):
                gat[2 * n + j, at, :] = g[:, j * 128 : (j + 1) * 128].astype(F32)

            @pl.when(y == 1)
            def _():
                halo_s[:, n * 256 : (n + 1) * 256] = g[half_rows - HALO :, :]

    def proj_glu_far(i):
        xin = unit_in(i)
        for n in range(chans // 256):
            g = gate(xin, n)
            for t in range(2):
                at = pl.ds(pl.multiple_of(HALO + yo * half_rows + t * rows + first_row(i), HALO), half_slot)
                part_g = g[t * half_slot : (t + 1) * half_slot]
                for j in range(2):
                    gat[2 * n + j, at, :] = part_g[:, j * 128 : (j + 1) * 128].astype(F32)
            if i == 0:

                @pl.when(yo == 1)
                def _():
                    halo_s[:, n * 256 : (n + 1) * 256] = g[rows - HALO : rows, :]

    def proj_q(h):
        xin = half_in(h)

        def one(n, c):
            q = dot(xin, wq[:, pl.ds(pl.multiple_of(n * 4 * hd, 4 * hd), 4 * hd)])
            qt = q.T.reshape(4, hd, half_rows)
            r = lax.rsqrt(jnp.mean(qt * qt, axis=1, keepdims=True) + 1e-06)
            qn = qt * r
            for j in range(2):
                gain = jnp.broadcast_to(q_gain[pl.ds(n * 2 + j, 1), :], (2 * hd, 2 * hd)).T
                for m in range(2):
                    gm = gain[m * hd : (m + 1) * hd, :half_rows]
                    val = (qn[j * 2 + m] * gm).astype(BF16).astype(F32) * (hd ** (-0.5) * LOG2_E)
                    high = val.astype(BF16)
                    low = (val - high.astype(F32)).astype(BF16)
                    first = (n * 2 + j) * tok + m * half_rows
                    lanes = pl.ds(pl.multiple_of(first, half_rows), half_rows)
                    qtz[h, m * hd : (m + 1) * hd, lanes] = high
                    qtz[h, (m + 2) * hd : (m + 3) * hd, lanes] = low
            return c

        for n in range(heads // 2):
            one(n, 0)

    def halo_copy():
        return pltpu.make_async_remote_copy(
            src_ref=halo_s,
            dst_ref=halo_r,
            send_sem=halo_sem.at[0],
            recv_sem=halo_sem.at[1],
            device_id=((sp + 1) % sp_n, tp),
            device_id_type=MESH,
        )

    def send_halo(h):
        @pl.when((sp < sp_n - 1) & (h == 1))
        def _():
            halo_copy().start()

    loaded(2, 5)
    ag_mate[0].wait_recv()
    proj_kv_near()
    for copy in ag_cross[2:]:
        copy.start()
    send_kv(0)
    loaded(5, 7)
    proj_glu_near()
    send_halo(y)
    loaded(7, 9)
    proj_q(y)

    def far_row(n):
        ag_cross[n].wait_recv()
        ag_fwd[n].start()

    far_row(0)
    far_row(1)
    ag_fwd[0].wait_recv()
    ag_fwd[1].wait_recv()
    proj_kv_far(0)
    send_kv(1)
    relay_last(0, 0, 1)
    relay_rest(0, 1, npos, across=False)
    far_row(2)

    @pl.when(core == 1)
    def _():
        far_row(3)

    proj_glu_far(0)
    send_halo(yo)
    @pl.when(core == 0)
    def _():
        far_row(3)

    relay_rest(0, 0, 1)
    relay_rest(0, 1, npos, along=False)
    relay_last(0, 1, 2)
    ag_fwd[2].wait_recv()
    ag_fwd[3].wait_recv()
    proj_kv_far(1)
    send_kv(2)
    proj_glu_far(1)
    def attend(blocks, q, diag, units=(0, 1, 2, 3)):
        keys = jnp.concatenate([kv[s, u, :rows, :] for s in blocks for u in units], axis=0)
        vals = jnp.concatenate([kv[s, u, rows:, :] for s in blocks for u in units], axis=0).T
        if diag:
            e = lax.broadcasted_iota(jnp.int32, (tok, 1), 0)
            kpos = e // half_rows * half_rows + e // half_slot % 2 * rows
            kpos = kpos + (1 - e // rows % 2) * half_slot + e % half_slot
            qpos = lax.broadcasted_iota(jnp.int32, (1, tok), 1)
            qpos = jnp.where(qpos >= half_rows, qpos - half_rows, qpos) + q * half_rows
            seen = kpos <= qpos
        every = dot(jnp.concatenate([keys, keys], axis=1), qtz[q])
        for h in range(heads):
            sc = every[:, h * tok : (h + 1) * tok]
            if diag:
                sc = jnp.where(seen, sc, -1e30)
                top = jnp.max(sc, axis=0, keepdims=True)
                wgt = jnp.exp2(sc - top)
                l_ref[h][q] = jnp.sum(wgt, axis=0, keepdims=True)
                acc[h][q] = dot(vals, wgt.astype(BF16))
            else:
                old = m_ref[h][q]
                top = jnp.maximum(old, jnp.max(sc, axis=0, keepdims=True))
                wgt = jnp.exp2(sc - top)
                alpha = jnp.exp2(old - top)
                l_ref[h][q] = l_ref[h][q] * alpha + jnp.sum(wgt, axis=0, keepdims=True)
                acc[h][q] = acc[h][q] * alpha + dot(vals, wgt.astype(BF16))
            m_ref[h][q] = top

    step_rows = 64
    loaded(9, 10)

    def conv_half(h):
        @pl.when((h == 0) & (sp > 0))
        def _():
            halo_copy().wait_recv()
            for j in range(chans // 128):
                gat[j, :HALO, :] = halo_r[:, j * 128 : (j + 1) * 128].astype(F32)

        @pl.when((h == 0) & (sp == 0))
        def _():
            gat[:, :HALO, :] = jnp.zeros((chans // 128, HALO, 128), F32)

        st[...] = jnp.zeros_like(st)

        def conv_cols(cc, c):
            cols = pl.ds(pl.multiple_of(cc * 128, 128), 128)
            rows_in = gat.at[cc, pl.ds(pl.multiple_of(h * half_rows, half_rows), HALO + half_rows), :]
            rows_out = conv.at[cc, pl.ds(pl.multiple_of(h * half_rows, half_rows), half_rows), :]
            for r0 in range(0, half_rows, step_rows):
                total = jnp.zeros((step_rows, 128), F32)
                for j in range(KW):
                    first = r0 + HALO - KW + 1 + j
                    total = total + taps[j : j + 1, cols] * rows_in[first : first + step_rows, :]
                rows_out[r0 : r0 + step_rows, :] = total
                st[0, r0 : r0 + step_rows, :] += total
                st[1, r0 : r0 + step_rows, :] += total * total
            return c

        lax.fori_loop(0, chans // 128, conv_cols, 0)
        stat[h, tp] = jnp.concatenate(
            [jnp.sum(st[i].T, axis=0, keepdims=True) for i in range(2)], axis=0
        )
        for i in range(1, tp_n):
            stat_copy(h, i).start()

    def stat_copy(h, i):
        return pltpu.make_async_remote_copy(
            src_ref=stat.at[h, tp],
            dst_ref=stat.at[h, tp],
            send_sem=stat_send.at[h, i],
            recv_sem=stat_recv.at[h, i],
            device_id=(sp, (tp + i) % tp_n),
            device_id_type=MESH,
        )

    wide = y_s.shape[2]
    chunks = width // wide

    def half_of(h):
        return pl.ds(pl.multiple_of(h * half_rows, half_rows), half_rows)

    def close_conv(h):
        for i in range(1, tp_n):
            stat_copy(h, i).wait_recv()
        sums = stat[h, 0]
        for i in range(1, tp_n):
            sums = sums + stat[h, i]
        sums = sums / (chans * tp_n)
        mu = sums[0:1]
        inv = lax.rsqrt(sums[1:2] - mu * mu + 1e-05)
        mu_t = jnp.broadcast_to(mu, (128, half_rows)).T
        inv_t = jnp.broadcast_to(inv, (128, half_rows)).T
        for cc in range(chans // 128):
            cols = slice(cc * 128, (cc + 1) * 128)
            val = (conv[cc, half_of(h), :] - mu_t) * inv_t * ln_gain[:, cols]
            c_out[half_of(h), cols] = (val * jax.nn.sigmoid(val)).astype(BF16)

    def out_conv(h):
        for n in range(chunks):
            cols = slice(n * wide, (n + 1) * wide)
            part[half_of(h), cols] = dot(c_out[half_of(h), :], woc[:, cols])

    relay_rest(1, 0, npos)
    relay_last(1, 0, 1)
    conv_half(yo)
    relay_last(1, 1, 2)
    tail = last & (lane == 0) & (pos > 0)

    @pl.when(jnp.logical_not(tail))
    def _():
        conv_half(y)

    relay_last(0, 2, npos)
    proj_q(yo)
    attend([sp], yo, True)
    relay_rest(2, 0, 1)
    relay_last(2, 0, 1)

    @pl.when(lane == 1)
    def _():
        for m in range(3):
            arrived(sp - 1, m)
        attend([sp - 1], yo, False)
        relay_last(1, 2, npos)
        relay_last(2, 1, npos)

    def near_attn():
        attend([sp], y, True)

        @pl.when(lane == 1)
        def _():
            attend([sp - 1], y, False)

    def near_conv():
        close_conv(y)
        out_conv(y)

    @pl.when(tail)
    def _():
        conv_half(y)

    relay_rest(2, 1, npos)
    @pl.when(lane == 0)
    def _():
        relay_last(1, 2, npos)
        relay_last(2, 1, npos)

    pl.when(pos > 0)(near_attn)


    def pairs_far():
        def one(i, c):
            p = pos - 1 - i
            for m in range(3):
                arrived(p * 2 + 1 - lane, m)
            attend([p * 2, p * 2 + 1], yo, False)
            return c

        ahead = jnp.where(tail, 1, 0)
        lax.fori_loop(0, ahead, one, 0)
        loaded(10, 11)
        close_conv(yo)
        loaded(11, 12)
        out_conv(yo)
        lax.fori_loop(ahead, pos, one, 0)

    def pairs_near():
        def one(i, c):
            p = pos - 1 - i
            attend([p * 2, p * 2 + 1], y, False)
            return c

        lax.fori_loop(0, pos, one, 0)

    loaded(12, 15)
    sub_t = jnp.broadcast_to(sub_gain[...], (half_rows, vdim)).T

    def close_heads(q):
        at = pl.ds(pl.multiple_of(q * half_rows, half_rows), half_rows)
        for h in range(heads):
            total = l_ref[h][q]
            log_row = m_ref[h][q] * LN_2 + jnp.log(total)
            maps = acc[h][q] / total
            for m in range(2):
                logs[m, h : h + 1, at] = log_row[:, m * half_rows : (m + 1) * half_rows]
            diff = maps[:, :half_rows] - lam[h] * maps[:, half_rows:]
            out = diff * lax.rsqrt(jnp.mean(diff * diff, axis=0, keepdims=True) + 1e-06) * sub_t
            a_out[at, h * vdim : (h + 1) * vdim] = out.T.astype(BF16)

    def mate_copy(k, n):
        return pltpu.make_async_remote_copy(
            src_ref=mate_s.at[k, n],
            dst_ref=mate_r.at[k, n],
            send_sem=mate_send.at[k, n],
            recv_sem=mate_recv.at[k, n],
            device_id=(sp, mate),
            device_id_type=MESH,
        )

    def y_copy(n):
        return pltpu.make_async_remote_copy(
            src_ref=y_s.at[n],
            dst_ref=y_r.at[n],
            send_sem=y_send.at[n],
            recv_sem=y_recv.at[n],
            device_id=(sp, cross),
            device_id_type=MESH,
        )

    def owner_rows(h, c):
        return pl.ds(pl.multiple_of((h * 2 + c) * rows, rows), rows)

    def out_attn(k, h):
        for piece in (range(0, 1), range(1, chunks)):
            for n in piece:
                cols = slice(n * wide, (n + 1) * wide)
                part[half_of(h), cols] += dot(a_out[half_of(h), :], woa[:, cols])
            for n in piece:
                cols = slice(n * wide, (n + 1) * wide)
                mate_s[k, n] = part[owner_rows(h, 1 - core), cols].astype(BF16)
                mate_copy(k, n).start()

    pairs_far()
    close_heads(yo)
    out_attn(0, yo)

    def forward(n, c):
        cols = pl.ds(pl.multiple_of(n * wide, wide), wide)
        mate_copy(0, n).wait_recv()
        y_s[n] = (part[owner_rows(yo, core), cols] + mate_r[0, n].astype(F32)).astype(BF16)
        y_copy(n).start()
        return c

    lax.fori_loop(0, chunks, forward, 0)

    @pl.when(pos == 0)
    def _():
        near_attn()

    near_conv()

    pairs_near()
    close_heads(y)
    out_attn(1, y)

    def finish(n, c):
        cols = pl.ds(pl.multiple_of(n * wide, wide), wide)
        mate_copy(1, n).wait_recv()
        y_copy(n).wait_recv()
        total = part[owner_rows(y, core), cols] + mate_r[1, n].astype(F32) + y_r[n].astype(F32)
        mixed[:, cols] = total.astype(BF16)
        return c

    for copy in ag_cross + ag_mate + ag_fwd:
        copy.wait_send()
    for h in range(2):
        for i in range(1, tp_n):
            stat_copy(h, i).wait_send()

    @pl.when(sp < sp_n - 1)
    def _():
        halo_copy().wait_send()

    for m in range(3):

        @pl.when(lane == 0)
        def _():
            x_copy(pos, m).wait_send()

        if m == late:
            direct_kv(lambda copy: copy.wait_send())
        else:
            tree_kv(pos, m, lambda copy: copy.wait_send())

        def relay_done(p, c):
            x_copy(p, m).wait_send()
            if m != late:
                tree_kv(p, m, lambda copy: copy.wait_send())
            return c

        lax.fori_loop(0, pos, relay_done, 0)
    lax.fori_loop(0, chunks, finish, 0)

    def rs_done(n, c):
        mate_copy(0, n).wait_send()
        mate_copy(1, n).wait_send()
        y_copy(n).wait_send()
        return c

    lax.fori_loop(0, chunks, rs_done, 0)


def put_out(mixed, logs, mixed_hbm, logs_hbm, sem):
    copies = [
        pltpu.make_async_copy(mixed, mixed_hbm, sem.at[0]),
        pltpu.make_async_copy(logs, logs_hbm, sem.at[1]),
    ]
    for copy in copies:
        copy.start()
    for copy in copies:
        copy.wait()


def on_device(sp_n, tp_n, *args):
    (
        tokens,
        norm_gain,
        w_glu_a,
        w_glu_b,
        conv_taps,
        ln_gain,
        w_query,
        w_key,
        w_value,
        query_gain,
        key_gain,
        lam_head,
        sub_gain,
        w_out_conv,
        w_out_attn,
    ) = args
    rows, width = tokens.shape
    tok = rows * tp_n
    half = tok // 2
    chans = conv_taps.shape[1]
    heads = lam_head.shape[0]
    qcols = w_query.shape[1]
    kcols = w_key.shape[1]
    vcols = w_value.shape[1]
    vdim = sub_gain.shape[0]
    acols = w_out_attn.shape[0]
    chunks = 4
    wide = width // chunks
    vmem = pl.BlockSpec(memory_space=pltpu.VMEM)
    dma = pltpu.SemaphoreType.DMA
    hbm = pl.BlockSpec(memory_space=pltpu.HBM)
    mixed, logs = pl.pallas_call(
        functools.partial(kernel, sp_n, tp_n),
        out_shape=(
            pltpu.VMEM((rows, width), BF16),
            pltpu.VMEM((2, heads, tok), F32),
        ),
        in_specs=[hbm] * 15,
        out_specs=(vmem, vmem),
        scratch_shapes=[
            pltpu.VMEM((rows, width), BF16),
            pltpu.VMEM((1, width), F32),
            pltpu.VMEM(conv_taps.shape, F32),
            pltpu.VMEM((1, chans), F32),
            pltpu.VMEM(query_gain.shape, F32),
            pltpu.VMEM(key_gain.shape, F32),
            pltpu.SMEM((heads,), F32),
            pltpu.VMEM((1, vdim), F32),
            pltpu.VMEM((width, chans), BF16),
            pltpu.VMEM((width, chans), BF16),
            pltpu.VMEM((width, qcols), BF16),
            pltpu.VMEM((width, kcols + vcols), BF16),
            pltpu.VMEM((chans, width), BF16),
            pltpu.VMEM((acols, width), BF16),
            pltpu.VMEM((tp_n, rows, width), BF16),
            pltpu.VMEM((sp_n, 4, 2 * rows, kcols), BF16),
            pltpu.VMEM((2, 2 * kcols, heads * tok), BF16),
            pltpu.VMEM((chans // 128, HALO + tok, 128), F32),
            pltpu.VMEM((HALO, chans), BF16),
            pltpu.VMEM((HALO, chans), BF16),
            pltpu.VMEM((chans // 128, tok, 128), F32),
            pltpu.VMEM((2, half, 128), F32),
            pltpu.VMEM((2, tp_n, 2, half), F32),
            pltpu.VMEM((tok, chans), BF16),
            [pltpu.VMEM((2, 1, tok), F32) for _ in range(heads)],
            [pltpu.VMEM((2, 1, tok), F32) for _ in range(heads)],
            [pltpu.VMEM((2, vdim, tok), F32) for _ in range(heads)],
            pltpu.VMEM((tok, acols), BF16),
            pltpu.VMEM((tok, width), F32),
            pltpu.VMEM((2, chunks, rows, wide), BF16),
            pltpu.VMEM((2, chunks, rows, wide), BF16),
            pltpu.VMEM((chunks, rows, wide), BF16),
            pltpu.VMEM((chunks, rows, wide), BF16),
            dma((15,)),
            dma((3, 4)),
            dma((3, 4)),
            dma((sp_n // 2, 3, max(2, sp_n // 2 - 1))),
            dma((sp_n // 2, 3)),
            dma((sp_n, 3)),
            dma((2,)),
            dma((2, tp_n)),
            dma((2, tp_n)),
            dma((2, chunks)),
            dma((2, chunks)),
            dma((chunks,)),
            dma((chunks,)),
        ],
        compiler_params=pltpu.CompilerParams(
            collective_id=0, has_side_effects=True, vmem_limit_bytes=56 * 2**20
        ),
    )(
        tokens,
        norm_gain.reshape(1, -1),
        w_glu_a,
        w_glu_b,
        conv_taps,
        ln_gain.reshape(1, -1),
        w_query,
        w_key,
        w_value,
        query_gain,
        key_gain,
        lam_head,
        sub_gain.reshape(1, -1),
        w_out_conv,
        w_out_attn,
    )
    return pl.pallas_call(
        put_out,
        out_shape=(
            jax.ShapeDtypeStruct((rows, width), BF16),
            jax.ShapeDtypeStruct((2, heads, tok), F32),
        ),
        in_specs=[vmem, vmem],
        out_specs=(hbm, hbm),
        scratch_shapes=[dma((2,))],
    )(
        pltpu.with_memory_space_constraint(mixed, pltpu.VMEM),
        pltpu.with_memory_space_constraint(logs, pltpu.VMEM),
    )


def solution(mesh):
    return jax.shard_map(
        functools.partial(on_device, mesh.shape["sp"], mesh.shape["tp"]),
        mesh=mesh,
        in_specs=(
            P(("sp", "tp"), None),
            P(),
            P(None, "tp"),
            P(None, "tp"),
            P(None, "tp"),
            P("tp"),
            P(None, "tp"),
            P(None, "tp"),
            P(None, "tp"),
            P("tp", None),
            P("tp", None),
            P("tp"),
            P(),
            P("tp", None),
            P("tp", None),
        ),
        out_specs=(P(("sp", "tp"), None), P(None, "tp", "sp")),
        check_vma=False,
    )
```
